32 devices in a mesh: sp: 16 (over z, y, x), tp: 2 (over core).
Axes of the slice: x: 2, y: 2, z: 4, core: 2. Of those that a mesh axis runs over, the one named last changes fastest.
Arguments:
- prompt: bfloat16 [16, 1024, 2048], P('sp', None, 'tp'), may hold values from -6 to 6
- new_input: bfloat16 [16, 2048], P('sp', 'tp'), may hold values from -140 to 140
- w_query: bfloat16 [2048, 2048], P('sp', 'tp'), may hold values from -0.21875 to 0.21875
- w_key: bfloat16 [2048, 2048], P('sp', 'tp'), may hold values from -0.125 to 0.125
- w_value: bfloat16 [2048, 2048], P('sp', 'tp'), may hold values from -0.125 to 0.125
- lam: float32 [16], P('tp'), may hold values from 0.3 to 0.8
- out_gain: float32 [128], replicated, may hold values from 0.1 to 1.9
Outputs:
- key_cache: bfloat16 [16, 1024, 2048], P('sp', None, 'tp')
- value_cache: bfloat16 [16, 1024, 2048], P('sp', None, 'tp')
- first_read: bfloat16 [16, 16, 128], P('sp', 'tp')
The draws below stay inside these ranges and needn't reach their ends.
All inputs are finite; a program needn't handle non-finite values.
Results may differ from the reference program's by a relative error of at most 0.02.
The reference program's roundings to bfloat16 on the way (of `query`) count: a program that leaves them out, or rounds other values in their place, can miss the bound.
Values may be sent and summed in bfloat16 or wider, within the bound.
A program may use at most 64 MiB of HBM per device.

```python
import jax
import jax.numpy as jnp
from jax import lax

WIDTH = 2048
HEADS = 16
MAP_DIM = 64
VAL_DIM = 128
LEN = 1024
SEQS = 16


def draw_new_input(key, part):
    values = jax.random.normal(key, (SEQS, WIDTH), jnp.float32)
    values = jnp.clip(values, -6.0, 6.0)
    return values.astype(jnp.bfloat16)


def levels(own_key, dims, shards, low, largest):
    gain = 1.0
    for dim, blocks in shards:
        draws = jax.random.uniform(jax.random.fold_in(jax.random.fold_in(own_key, 6), dim), (blocks,), jnp.float32, low / len(shards), largest / len(shards))
        gain = gain * jnp.repeat(jnp.exp(draws), dims[dim] // blocks).reshape((-1,) + (1,) * (len(dims) - 1 - dim))
    return gain


def gaussian(own_key, shape, width, reach, split=(), kind=jnp.bfloat16):
    level = levels(own_key, shape, split, -0.22, 0.18) if split else 1.0
    drawn = jax.random.normal(own_key, shape, jnp.float32) * width * level
    return jnp.minimum(jnp.maximum(drawn, -reach), reach).astype(kind)


def setup_inputs(seed: int = 0) -> dict:
    streams_of = jax.random.split(jax.random.key(seed), 8)
    prompt = gaussian(streams_of[0], (SEQS, LEN, WIDTH), 1.0, 6.0, ((0, 16), (2, 2)))
    new_input = draw_new_input(jax.random.fold_in(streams_of[7], 71), 0)
    w_query = gaussian(streams_of[2], (WIDTH, HEADS * 2 * MAP_DIM), (WIDTH // 3) ** -0.5, 0.21875, ((0, 16), (1, 2)))
    w_key = gaussian(streams_of[3], (WIDTH, HEADS * 2 * MAP_DIM), WIDTH ** -0.5, 0.125, ((0, 16), (1, 2)))
    w_value = gaussian(streams_of[4], (WIDTH, HEADS * VAL_DIM), WIDTH ** -0.5, 0.125, ((0, 16), (1, 2)))
    lam = jnp.clip(0.3 + 0.5 * jax.random.uniform(streams_of[5], (HEADS,), jnp.float32) ** levels(streams_of[5], (HEADS,), ((0, 2),), -0.2, 0.2), 0.3, 0.8)
    out_gain = jnp.clip(1.0 + 0.18 * jax.random.normal(streams_of[6], (VAL_DIM,), jnp.float32), 0.1, 1.9)
    return {"prompt": prompt, "new_input": new_input, "w_query": w_query, "w_key": w_key, "w_value": w_value, "lam": lam, "out_gain": out_gain}


rope_base = 500000.0
norm_eps = 1e-05

def rotate(vectors, angle):
    half = vectors.shape[-1] // 2
    cosine_table = jnp.cos(angle)
    sine = jnp.sin(angle)
    first = vectors[..., :half]
    second = vectors[..., half:]
    return jnp.concatenate([first * cosine_table - second * sine, second * cosine_table + first * sine], axis=-1)

def inverse_freq():
    return rope_base ** (-(jnp.arange(MAP_DIM // 2, dtype=jnp.float32) * 2.0 / MAP_DIM))

def reference(prompt, new_input, w_query, w_key, w_value, lam, out_gain):
    rows = prompt.reshape(SEQS * LEN, WIDTH)
    inverse = inverse_freq()
    positions = jnp.arange(LEN, dtype=jnp.float32)
    keys = jnp.dot(rows, w_key, preferred_element_type=jnp.float32).reshape(SEQS, LEN, HEADS, 2, MAP_DIM)
    keys = rotate(keys, positions[:, None, None, None] * inverse).astype(jnp.bfloat16)
    values = jnp.dot(rows, w_value, preferred_element_type=jnp.float32).astype(jnp.bfloat16)
    values = values.reshape(SEQS, LEN, HEADS, VAL_DIM)
    query = jnp.dot(new_input, w_query, preferred_element_type=jnp.float32).reshape(SEQS, HEADS, 2, MAP_DIM)
    query = rotate(query, jnp.float32(LEN) * inverse).astype(jnp.bfloat16)

    def single_sequence(args):
        single_head_query, single_head_keys, single_head_values = args
        attention_scores = jnp.einsum('fke,afke->fka', single_head_query.astype(jnp.float32), single_head_keys.astype(jnp.float32))
        weights = jax.nn.softmax(attention_scores * MAP_DIM ** (-0.5), axis=-1)
        mixed = jnp.einsum('hml,lhe->hme', weights, single_head_values.astype(jnp.float32), precision=lax.Precision.HIGHEST)
        diff = mixed[:, 0] - lam[:, None] * mixed[:, 1]
        normed = diff * lax.rsqrt(lax.optimization_barrier(jnp.mean(diff * diff, axis=-1, keepdims=True)) + norm_eps)
        return (normed * out_gain).astype(jnp.bfloat16)
    first_read = lax.map(single_sequence, (query, keys, values))
    return (keys.reshape(SEQS, LEN, HEADS * 2 * MAP_DIM), values.reshape(SEQS, LEN, HEADS * VAL_DIM), first_read)
```

```python
import functools
import math

import jax
import jax.numpy as jnp
from jax import lax
from jax.experimental import pallas as pl
from jax.experimental.pallas import tpu as pltpu
from jax.sharding import PartitionSpec as P

MAP_DIM = 64
VAL_DIM = 128
LANES = 128
rope_base = 500000.0
norm_eps = 1e-05

X, Y, UP, DOWN = 0, 1, 2, 3
F32, BF16 = jnp.float32, jnp.bfloat16


def inverse_freq(shape):
    lane = lax.broadcasted_iota(jnp.int32, shape, 1) % (MAP_DIM // 2)
    return jnp.exp(lane.astype(F32) * (-2.0 / MAP_DIM * math.log(rope_base)))


def table(position):
    angle = position * inverse_freq(position.shape)
    lane = lax.broadcasted_iota(jnp.int32, angle.shape, 1) % MAP_DIM
    sine = jnp.sin(angle)
    return jnp.cos(angle), jnp.where(lane < MAP_DIM // 2, -sine, sine)


def rotated(tile, cosine, sine):
    half = MAP_DIM // 2
    lane = lax.broadcasted_iota(jnp.int32, tile.shape, 1) % MAP_DIM
    other = jnp.where(lane < half, pltpu.roll(tile, LANES - half, 1), pltpu.roll(tile, half, 1))
    return tile * cosine + other * sine


def groups(cols):
    return max(g for g in (4, 2, 1) if cols % (g * LANES) == 0)


def kernel(
    n, tp, G, heads, prompt, fresh, wq, wk, wv, lam, gain,
    k_out, v_out, mix_out, gain_out,
    W, PR, acc, fr, XN, XM, wq_v, QS, QR, ct, st, qs, lam_v,
    w_recv, w_send, p_recv, p_send, x_recv, x_send, xt_recv, xt_send, q_recv, q_send, loc, token,
):
    _, rows, wl = prompt.shape
    depth, cols = wk.shape
    width = cols // G
    L = n // 4
    plane = 4 * depth
    me, mt = lax.axis_index("sp"), lax.axis_index("tp")
    z, y, x = me // 4, (me // 2) % 2, me % 2
    yf, xf = 1 - y, 1 - x
    up_ok, down_ok = z + 1 < L, z > 0
    outer = jnp.logical_not(up_ok & down_ok)

    first = [X if j < (G + 1) // 2 else Y for j in range(G)]
    second = [X + Y - f for f in first]
    wide = [G >= 4 and j % 2 == 1 for j in range(G)]
    order = [j for j in range(G) if not wide[j]] + [j for j in range(G) if wide[j]]
    wides = [j for j in range(G) if wide[j]]

    def at(zo, yo, xo):
        return zo * 4 + yo * 2 + xo

    def across(zo, axis):
        return at(zo, y, xf) if axis == X else at(zo, yf, x)

    partner = {X: at(z, y, xf), Y: at(z, yf, x), UP: me + 4, DOWN: me - 4}

    def piece(c, o):
        return W.at[c, pl.ds(pl.multiple_of(o * depth, depth), depth), :]

    def copy(c, d, o):
        return pltpu.make_async_remote_copy(
            src_ref=piece(c, o), dst_ref=piece(c, o),
            send_sem=w_send.at[d], recv_sem=w_recv.at[c * n + o],
            device_id={"sp": partner[d]}, device_id_type=pl.DeviceIdType.MESH,
        )

    def got(c, o):
        copy(c, X, o).wait_recv()

    def hop(c, o, dirs, wait=True):
        if wait:
            got(c, o)
        for d, ok in dirs:
            if ok is None:
                copy(c, d, o).start()
            else:
                pl.when(ok)(lambda d=d: copy(c, d, o).start())

    def own_sends(m):
        for j in range(G):
            hop(m * G + j, me, [(X, None), (UP, up_ok), (DOWN, down_ok)], wait=False)
        for j in sorted(range(G), key=lambda j: first[j] != Y):
            hop(m * G + j, me, [(Y, None)], wait=False)

    def in_plane(m, zo, along=()):
        for j in range(G):
            hop(m * G + j, across(zo, first[j]), list(along) + [(second[j], None)])

    def own_plane(m):
        in_plane(m, z, [(UP, outer & up_ok), (DOWN, outer & down_ok)])

    def own_wide(m):
        if not wides:
            return

        @pl.when(outer)
        def _():
            for other in (True, False):
                for j in wides:
                    o = across(z, second[j]) if other else at(z, yf, xf)
                    hop(m * G + j, o, [(UP, up_ok), (DOWN, down_ok)])

    def block(m, b, upper=True, lower=True):
        sides = [(z + 1 + b, L - 1 - z, down_ok, DOWN)] * upper + [(z - 1 - b, z, up_ok, UP)] * lower
        for zo, e, more, d in sides:
            if b < L - 2:
                @pl.when(b < e - 1)
                def _(zo=zo, more=more, d=d):
                    for j in order:
                        hop(m * G + j, at(zo, y, x), [(d, more), (first[j], None), (second[j], None)])
            end = 0 if d == UP else L - 1
            if b < L - 1:
                @pl.when(b == e - 1)
                def _(end=end, more=more, d=d):
                    for j in order:
                        far = [] if wide[j] else [(second[j], None)]
                        hop(m * G + j, at(end, y, x), [(d, more)] + far)
            if 1 <= b < L:
                @pl.when((b == e) & (e > 0))
                def _(end=end, more=more, d=d):
                    for j in order:
                        far = [] if wide[j] else [(second[j], None)]
                        hop(m * G + j, across(end, first[j]), [(d, more)] + far)
            if 2 <= b and wides:
                @pl.when((b == e + 1) & (e > 0))
                def _(end=end, more=more, d=d):
                    for other in (True, False):
                        for j in wides:
                            o = across(end, second[j]) if other else at(end, yf, xf)
                            hop(m * G + j, o, [(d, more)])

    def in_plane_of(m, s):
        if not 1 <= s <= L - 2:
            return
        for zo, ok in ((z + s, z + s < L - 1), (z - s, z - s > 0)):
            pl.when(ok)(lambda zo=zo: in_plane(m, zo))

    def loop(lo, hi, f):
        lax.fori_loop(lo, hi, lambda i, _: (f(i), _)[1], 0)

    R = min(rows, 512)

    near = jnp.minimum(z, L - 1 - z)
    far = jnp.where(z < L - 1 - z, 1, -1)

    def dots(m, t, last=False):
        turn = (t + 1) // 2 if t % 2 else -(t // 2)
        zo = z + far * jnp.where(t <= 2 * near, turn, t - near)
        thin = (zo > 0) & (zo < L - 1)
        for j in range(G):
            def rest_of(j=j):
                got(m * G + j, across(zo, second[j]))
                got(m * G + j, at(zo, yf, xf))
            if wide[j]:
                pl.when(thin)(rest_of)
            else:
                rest_of()

        def tile(i):
            r = pl.ds(pl.multiple_of(i * R, R), R)
            p = pl.ds(pl.multiple_of(zo * plane, plane), plane)
            for j in range(G):
                part = jnp.dot(PR[r, p], W[m * G + j, p, :], preferred_element_type=F32)
                if t > 0:
                    part = acc[j, r, :] + part
                if last:
                    v_out[r, pl.ds(j * width, width)] = part.astype(BF16)
                else:
                    acc[j, r, :] = part

        loop(0, rows // R, tile)

    barrier = pltpu.get_barrier_semaphore()
    for d in range(1, tp):
        pl.semaphore_signal(
            barrier, inc=1, device_id={"tp": (mt + d) % tp}, device_id_type=pl.DeviceIdType.MESH)

    def signal(sem, d):
        pl.semaphore_signal(
            sem, inc=1, device_id={"sp": partner[d]}, device_id_type=pl.DeviceIdType.MESH)

    signal(barrier, X)
    signal(barrier, Y)
    pl.when(up_ok)(lambda: signal(barrier, UP))
    pl.when(down_ok)(lambda: signal(barrier, DOWN))

    def columns(t):
        return PR.at[:, pl.ds(pl.multiple_of(t * wl, wl), wl)]

    own = [
        pltpu.make_async_copy(
            w.at[:, pl.ds(j * width, width)], piece(m * G + j, me), loc.at[m])
        for m, w in enumerate((wk, wv)) for j in range(G)
    ]
    rest = [
        pltpu.make_async_copy(src, dst, loc.at[2 + i])
        for i, (src, dst) in enumerate((
            (fresh, fr), (prompt.at[0], columns(mt)), (wq, wq_v), (lam, lam_v), (gain, gain_out)))
    ]

    def own_wait(m):
        whole = W.at[pl.ds(m * G, G), pl.ds(pl.multiple_of(me * depth, depth), depth), :]
        pltpu.make_async_copy(whole, whole, loc.at[m]).wait()

    for c in own[:G]:
        c.start()
    rest[0].start()
    for c in own[G:]:
        c.start()
    for c in rest[1:]:
        c.start()
    own_wait(0)

    @pl.when(up_ok & down_ok)
    def _():
        pl.semaphore_wait(barrier, 4 + tp - 1)

    @pl.when(outer)
    def _():
        pl.semaphore_wait(barrier, 3 + tp - 1)

    own_sends(0)

    def x_copy(d):
        return pltpu.make_async_remote_copy(
            src_ref=XN.at[mt, me], dst_ref=XN.at[mt, me],
            send_sem=x_send.at[0], recv_sem=x_recv.at[0],
            device_id={"sp": (me + d) % n}, device_id_type=pl.DeviceIdType.MESH,
        )

    def together(ref, send_sem, recv_sem):
        return pltpu.make_async_remote_copy(
            src_ref=ref, dst_ref=ref, send_sem=send_sem.at[0], recv_sem=recv_sem.at[0],
            device_id={"sp": partner[X]}, device_id_type=pl.DeviceIdType.MESH,
        )

    x_all = together(XN.at[0, pl.ds(0, n - 1)], x_send, x_recv)
    q_all = together(QR.at[pl.ds(0, n - 1)], q_send, q_recv)

    def p_copy(d):
        return pltpu.make_async_remote_copy(
            src_ref=prompt.at[0], dst_ref=columns(mt),
            send_sem=p_send.at[d], recv_sem=p_recv.at[mt],
            device_id={"tp": (mt + d) % tp}, device_id_type=pl.DeviceIdType.MESH,
        )

    def p_wait(d):
        src = (mt + d) % tp
        return pltpu.make_async_remote_copy(
            src_ref=columns(src), dst_ref=columns(src),
            send_sem=p_send.at[d], recv_sem=p_recv.at[src],
            device_id={"tp": src}, device_id_type=pl.DeviceIdType.MESH,
        )

    signal(token.at[Y], Y)

    def relay_token(b):
        for turn, before, more, d in ((z == b, down_ok, up_ok, UP), (z == L - 1 - b, up_ok, down_ok, DOWN)):
            pl.when(turn & before)(lambda d=d: pl.semaphore_wait(token.at[d], 1))
            pl.when(turn & more)(lambda d=d: signal(token.at[d], d))

    rest[0].wait()
    XN[mt, me] = fr[...].astype(F32)
    own_wait(1)
    for d in range(1, tp):
        p_copy(d).start()


    def xt_copy(d, t):
        return pltpu.make_async_remote_copy(
            src_ref=XN.at[t], dst_ref=XN.at[t],
            send_sem=xt_send.at[d], recv_sem=xt_recv.at[t],
            device_id={"tp": (mt + d) % tp}, device_id_type=pl.DeviceIdType.MESH,
        )

    def q_copy(d):
        dst = (me + d) % n
        return pltpu.make_async_remote_copy(
            src_ref=QS.at[dst], dst_ref=QR.at[me],
            send_sem=q_send.at[0], recv_sem=q_recv.at[0],
            device_id={"sp": dst}, device_id_type=pl.DeviceIdType.MESH,
        )

    def share_new():
        x_all.wait_recv()
        for d in range(1, tp):
            xt_copy(d, mt).start()

    def partial_queries():
        for d in range(1, tp):
            xt_copy(d, (mt + d) % tp).wait_recv()
        begin = me * depth
        holder, offset = begin // wl, begin % wl
        for j in range(n):
            XM[pl.ds(j, 1), :] = XN[holder, j]
        pick = (
            lax.broadcasted_iota(jnp.int32, (wl, depth), 0)
            == offset + lax.broadcasted_iota(jnp.int32, (wl, depth), 1)
        )
        chosen = jnp.dot(
            XM[...].astype(BF16), jnp.where(pick, 1.0, 0.0).astype(BF16), preferred_element_type=F32
        ).astype(BF16)
        rest[2].wait()
        partial = jnp.dot(chosen, wq_v[...], preferred_element_type=F32)
        for j in range(n):
            QS[j] = partial[j:j + 1, :]
        QR[me] = QS[me]
        loop(1, n, lambda d: q_copy(d).start())

    hp = max(heads, 8)
    pad = 2 * hp

    def build_query():
        qcos, qsin = table(jnp.full((8, LANES), rows, F32))
        q_all.wait_recv()
        total = QR[0]
        for j in range(1, n):
            total = total + QR[j]
        total = jnp.broadcast_to(total, (8, cols))
        query = jnp.concatenate(
            [rotated(total[:, i:i + LANES], qcos, qsin) for i in range(0, cols, LANES)], axis=1)
        query = jnp.broadcast_to(query[:1], (pad, cols))
        row = lax.broadcasted_iota(jnp.int32, (pad, cols), 0)
        keep = 2 * (row % hp) + row // hp == lax.broadcasted_iota(jnp.int32, (pad, cols), 1) // MAP_DIM
        qs[...] = jnp.where(keep, query, 0.0).astype(BF16)

    def angles(i):
        position = (i * 64 + lax.broadcasted_iota(jnp.int32, (64, LANES), 0)).astype(F32)
        r = pl.ds(pl.multiple_of(i * 64, 64), 64)
        ct[r, :], st[r, :] = table(position)

    RR = min(rows, 256)

    def rotate_rows(i):
        r = pl.ds(pl.multiple_of(i * RR, RR), RR)
        cosine, sine = ct[r, :], st[r, :]
        for i in range(0, cols, LANES):
            tile = acc[i // width, r, pl.ds(i % width, LANES)]
            k_out[r, pl.ds(i, LANES)] = rotated(tile, cosine, sine).astype(BF16)

    def weigh():
        scores = lax.dot_general(
            qs[...], k_out[...], (((1,), (1,)), ((), ())), preferred_element_type=F32) * MAP_DIM ** -0.5
        weights = jnp.exp(scores - jnp.max(scores, axis=-1, keepdims=True))
        weights = weights / jnp.sum(weights, axis=-1, keepdims=True)
        rest[3].wait()
        here = (lax.broadcasted_iota(jnp.int32, (hp, heads), 0)
                == lax.broadcasted_iota(jnp.int32, (hp, heads), 1))
        scale = jnp.sum(jnp.where(here, lam_v[...], 0.0), axis=-1, keepdims=True)
        mix = weights[:hp] - scale * weights[hp:]
        high = mix.astype(BF16)
        left = mix - high.astype(F32)
        mid = left.astype(BF16)
        low = (left - mid.astype(F32)).astype(BF16)
        mix_out[...] = jnp.concatenate([high, mid, low], axis=0)

    own_plane(0)
    pl.semaphore_wait(token.at[Y], 1)
    signal(token.at[X], X)
    steps = iter(range(L))

    def pass_token():
        for b in steps:
            relay_token(b)
            break

    block(0, 0, upper=True, lower=False)
    pl.semaphore_wait(token.at[X], 1)
    pass_token()
    block(0, 0, upper=False)
    pass_token()
    own_wide(0)
    pass_token()
    for b in range(1, L + 1):
        block(0, b, lower=False)
        pass_token()
        block(0, b, upper=False)
        if b == 1:
            own_sends(1)
        in_plane_of(0, b)
        if b == max(1, L - 3):
            for k in steps:
                relay_token(k)
            loop(1, n, lambda d: x_copy(d).start())
        if b == 1:
            own_plane(1)
            rest[1].wait()
            for d in range(1, tp):
                p_wait(d).wait_recv()
            dots(0, 0)
        if b == min(2, L):
            own_wide(1)
        if b == min(3, L):
            loop(0, rows // 64, angles)
            share_new()
        if b >= 3:
            dots(0, b - 2)

    partial_queries()
    for b in range(L + 1):
        if b == L > 2:
            dots(1, L - 2)
        block(1, b)
        in_plane_of(1, b)
        if b == 0:
            if L > 1:
                dots(0, L - 1)
            loop(0, rows // RR, rotate_rows)
        if b == 1 and L > 1:
            dots(1, 0)
        if b == min(2, L):
            build_query()
            weigh()
        if 3 <= b < L:
            dots(1, b - 2)
    dots(1, L - 1, last=True)
    rest[4].wait()
    x_all.wait_send()
    q_all.wait_send()
    for d in range(1, tp):
        p_copy(d).wait_send()
        xt_copy(d, mt).wait_send()

    def sent(d, pieces):
        all_of = W.at[:, pl.ds(0, pieces * depth // G), :]
        pltpu.make_async_remote_copy(
            src_ref=all_of, dst_ref=all_of, send_sem=w_send.at[d], recv_sem=w_recv.at[0],
            device_id={"sp": partner[X]}, device_id_type=pl.DeviceIdType.MESH,
        ).wait_send()

    def plane_pieces(d, inner, outers):
        turned = sum(s == d for s in second)
        halves = 2 * sum(s == d and not w for s, w in zip(second, wide))
        return (inner + 1) * (G + turned) + outers * halves

    def settle(inner, outers):
        for d in (X, Y):
            sent(d, plane_pieces(d, inner, outers))

    pl.when(outer)(lambda: settle(max(L - 2, 0), min(L - 1, 1)))
    if L > 2:
        pl.when(jnp.logical_not(outer))(lambda: settle(L - 3, 2))
    total = 0
    for k in range(L - 1):
        total += G if 0 < k else 2 * G + 2 * len(wides)
        pl.when(z == k)(lambda total=total: sent(UP, total))
        pl.when(z == L - 1 - k)(lambda total=total: sent(DOWN, total))


def read(keys, values, mix, gain, k_out, v_out, read_out, sem):
    hp = mix.shape[0] // 3
    heads = read_out.shape[1]
    k_copy = pltpu.make_async_copy(keys, k_out.at[0], sem.at[0])
    v_copy = pltpu.make_async_copy(values, v_out.at[0], sem.at[1])
    v_copy.start()
    k_copy.start()
    mixed = jnp.dot(mix[...], values[...], preferred_element_type=F32)
    mixed = mixed[:hp] + mixed[hp:2 * hp] + mixed[2 * hp:]
    diff = jnp.concatenate(
        [mixed[h:h + 1, h * VAL_DIM:(h + 1) * VAL_DIM] for h in range(heads)], axis=0)
    normed = diff * lax.rsqrt(jnp.mean(diff * diff, axis=-1, keepdims=True) + norm_eps)
    read_out[0] = (normed * gain[...]).astype(BF16)
    v_copy.wait()
    k_copy.wait()


def body(n, tp, prompt, new_input, w_query, w_key, w_value, lam, out_gain):
    seqs, rows, wl = prompt.shape
    depth, cols = w_key.shape
    heads = lam.shape[0]
    G = groups(cols)
    hp = max(heads, 8)
    operands = [
        pltpu.with_memory_space_constraint(a, pltpu.HBM)
        for a in (prompt, new_input, w_query, w_key, w_value, lam[None, :], out_gain[None, :])
    ]
    any_ = pl.BlockSpec(memory_space=pl.ANY)
    hbm = pl.BlockSpec(memory_space=pltpu.HBM)
    vmem = pl.BlockSpec(memory_space=pltpu.VMEM)
    dma = pltpu.SemaphoreType.DMA
    keys, values, mix, gain = pl.pallas_call(
        functools.partial(kernel, n, tp, G, heads),
        out_shape=(
            pltpu.VMEM((rows, cols), BF16),
            pltpu.VMEM((rows, cols), BF16),
            pltpu.VMEM((3 * hp, rows), BF16),
            pltpu.VMEM((1, VAL_DIM), F32),
        ),
        in_specs=[hbm] * 7,
        out_specs=(vmem, vmem, vmem, vmem),
        scratch_shapes=[
            pltpu.VMEM((2 * G, n * depth, cols // G), BF16),
            pltpu.VMEM((rows, tp * wl), BF16),
            pltpu.VMEM((G, rows, cols // G), F32),
            pltpu.VMEM((1, wl), BF16),
            pltpu.VMEM((tp, n, 1, wl), F32),
            pltpu.VMEM((n, wl), F32),
            pltpu.VMEM((depth, cols), BF16),
            pltpu.VMEM((n, 1, cols), F32),
            pltpu.VMEM((n, 1, cols), F32),
            pltpu.VMEM((rows, LANES), F32),
            pltpu.VMEM((rows, LANES), F32),
            pltpu.VMEM((2 * hp, cols), BF16),
            pltpu.VMEM((1, heads), F32),
            dma((2 * G * n,)), dma((4,)), dma((tp,)), dma((tp,)), dma((1,)), dma((1,)),
            dma((tp,)), dma((tp,)), dma((1,)), dma((1,)), dma((7,)),
            pltpu.SemaphoreType.REGULAR((4,)),
        ],
        compiler_params=pltpu.CompilerParams(
            collective_id=0, has_side_effects=True, vmem_limit_bytes=44 * 1024 * 1024),
        name="prefill",
    )(*operands)
    return pl.pallas_call(
        read,
        out_shape=(
            jax.ShapeDtypeStruct((seqs, rows, cols), BF16),
            jax.ShapeDtypeStruct((seqs, rows, cols), BF16),
            jax.ShapeDtypeStruct((seqs, heads, VAL_DIM), BF16),
        ),
        in_specs=[vmem] * 4,
        out_specs=(any_, any_, vmem),
        scratch_shapes=[dma((2,))],
        compiler_params=pltpu.CompilerParams(vmem_limit_bytes=24 * 1024 * 1024),
        name="read",
    )(keys, values, mix, gain)


def solution(mesh):
    in_specs = (
        P("sp", None, "tp"), P("sp", "tp"), P("sp", "tp"), P("sp", "tp"), P("sp", "tp"), P("tp"), P(),
    )
    out_specs = (P("sp", None, "tp"), P("sp", None, "tp"), P("sp", "tp", None))
    return jax.shard_map(
        functools.partial(body, mesh.shape["sp"], mesh.shape["tp"]),
        mesh=mesh, in_specs=in_specs, out_specs=out_specs, check_vma=False)
```

```python
import functools
import heapq
import math

import jax
import jax.numpy as jnp
from jax import lax
from jax.experimental import pallas as pl
from jax.experimental.pallas import tpu as pltpu
from jax.sharding import PartitionSpec as P

MAP_DIM = 64
VAL_DIM = 128
LANES = 128
rope_base = 500000.0
norm_eps = 1e-05

X, Y, UP, DOWN = 0, 1, 2, 3
LAG, LEAD = 0.9, 3.0
TOK0, TOK1 = 2.5, 4.0
F32, BF16 = jnp.float32, jnp.bfloat16


def inverse_freq(shape):
    lane = lax.broadcasted_iota(jnp.int32, shape, 1) % (MAP_DIM // 2)
    return jnp.exp(lane.astype(F32) * (-2.0 / MAP_DIM * math.log(rope_base)))


def table(position):
    angle = position * inverse_freq(position.shape)
    lane = lax.broadcasted_iota(jnp.int32, angle.shape, 1) % MAP_DIM
    sine = jnp.sin(angle)
    return jnp.cos(angle), jnp.where(lane < MAP_DIM // 2, -sine, sine)


def rotated(tile, cosine, sine):
    half = MAP_DIM // 2
    lane = lax.broadcasted_iota(jnp.int32, tile.shape, 1) % MAP_DIM
    other = jnp.where(lane < half, pltpu.roll(tile, LANES - half, 1), pltpu.roll(tile, half, 1))
    return tile * cosine + other * sine


def groups(cols):
    return max(g for g in (4, 2, 1) if cols % (g * LANES) == 0)


class Plan:
    def __init__(self, L, G):
        self.L, self.G = L, G
        self.first = [X if j < (G + 1) // 2 else Y for j in range(G)]
        self.wide = [G >= 4 and j % 2 == 1 for j in range(G)]
        self.arrival = [{} for _ in range(L)]
        self.start = [{} for _ in range(L)]
        waiting = {(z, d): [] for z in range(L) for d in range(4)}
        free = dict.fromkeys(waiting, 0.0)
        events, count = [], 0

        def post(time, what):
            nonlocal count
            count += 1
            heapq.heappush(events, (time, count, what))

        def begin(z, d, time):
            if waiting[z, d] and free[z, d] <= time:
                piece = heapq.heappop(waiting[z, d])[-1]
                self.start[z][piece, d] = time
                free[z, d] = time + 1
                post(time + 1, (z, d, None))
                post(time + 1 + LAG, (*self.beyond(z, piece, d)[:1], None, self.beyond(z, piece, d)[1]))

        for z in range(L):
            for m in range(2):
                for j in range(G):
                    post(0.0, (z, None, (m, j, z, 0, 0)))
        while events:
            time, _, (z, d, piece) = heapq.heappop(events)
            if d is not None:
                begin(z, d, time)
                continue
            assert piece not in self.arrival[z]
            self.arrival[z][piece] = time
            for d in self.links(z, piece):
                count += 1
                goes_on = bool(self.links(*self.beyond(z, piece, d)))
                heapq.heappush(waiting[z, d], (self.rank(z, piece, d), count, piece))
            for d in range(4):
                begin(z, d, time)
        self.end = max(max(a.values()) for a in self.arrival)

    def rank(self, z, piece, d):
        m, j, zo, dy, dx = piece
        there, seen = self.beyond(z, piece, d)
        relayed = any(link in (X, Y) for link in self.links(there, seen))
        return m, not relayed

    def outer(self, zo):
        return zo in (0, self.L - 1)

    def links(self, z, piece):
        m, j, zo, dy, dx = piece
        along = [d for d, step in ((UP, 1), (DOWN, -1))
                 if 0 <= z + step < self.L and (z == zo or (step > 0) == (z > zo))]
        second = [X + Y - self.first[j]]
        if (dy, dx) == (0, 0):
            if z == zo or not self.outer(zo):
                return along + [X, Y]
            return along + second * (not self.wide[j])
        if (dx if self.first[j] == X else dy) and not (dx and dy):
            along = along * self.outer(zo)
            return along + second * (z == zo or not self.outer(zo) or not self.wide[j])
        return along * (self.outer(zo) and self.wide[j])

    def beyond(self, z, piece, d):
        m, j, zo, dy, dx = piece
        return z + (d == UP) - (d == DOWN), (m, j, zo, dy ^ (d == Y), dx ^ (d == X))

    def roles(self):
        return range((self.L + 1) // 2)

    def sends(self, k):
        own = ((max(self.arrival[k][p], t - LEAD), t, p, d) for (p, d), t in self.start[k].items())
        return [(when, p, d) for when, _, p, d in sorted(own)]

    def pieces(self, m, zo, groups):
        return [(m, j, zo, dy, dx) for j in groups for dy in range(2) for dx in range(2)]

    def ready(self, k, m, zo, groups):
        return max(self.arrival[k][p] for p in self.pieces(m, zo, groups))

    def order(self, k, m):
        everything = range(self.G)
        return sorted(range(self.L), key=lambda zo: (zo != k, self.ready(k, m, zo, everything)))


def kernel(
    n, tp, G, heads, prompt, fresh, wq, wk, wv, lam, gain,
    k_out, v_out, mix_out, gain_out,
    W, PR, acc, fr, XR, XM, wq_v, QS, QR, ct, st, qs, lam_v,
    w_recv, w_send, p_recv, p_send, x_recv, x_send, q_recv, q_send, loc, token,
):
    _, rows, wl = prompt.shape
    depth, cols = wk.shape
    width = cols // G
    L = n // 4
    plane = 4 * depth
    me, mt = lax.axis_index("sp"), lax.axis_index("tp")
    z, y, x = me // 4, (me // 2) % 2, me % 2
    yf, xf = 1 - y, 1 - x
    up_ok, down_ok = z + 1 < L, z > 0
    outer = jnp.logical_not(up_ok & down_ok)

    plan = Plan(L, G)
    role = jnp.minimum(z, L - 1 - z)
    ahead = jnp.where(z <= L - 1 - z, 1, -1)

    def at(zo, yo, xo):
        return zo * 4 + yo * 2 + xo

    partner = {X: at(z, y, xf), Y: at(z, yf, x), UP: me + 4, DOWN: me - 4}

    def piece(c, o):
        return W.at[c, pl.ds(pl.multiple_of(o * depth, depth), depth), :]

    target = {X: partner[X], Y: partner[Y], UP: me + 4 * ahead, DOWN: me - 4 * ahead}

    def place(k, p):
        m, j, zo, dy, dx = p
        return m * G + j, at(z + ahead * (zo - k), yf if dy else y, xf if dx else x)

    def copy(c, d, o):
        return pltpu.make_async_remote_copy(
            src_ref=piece(c, o), dst_ref=piece(c, o),
            send_sem=w_send.at[d], recv_sem=w_recv.at[c * n + o],
            device_id={"sp": target[d]}, device_id_type=pl.DeviceIdType.MESH,
        )

    def by_role(f):
        for k in plan.roles():
            pl.when(role == k)(functools.partial(f, k))

    pending = {k: plan.sends(k) for k in plan.roles()}
    arrived = {k: set(plan.pieces(0, k, range(0))) for k in plan.roles()}

    def need(k, p):
        if p[2:] != (k, 0, 0) and p not in arrived[k]:
            arrived[k].add(p)
            c, o = place(k, p)
            copy(c, X, o).wait_recv()

    def advance(time, wanted=lambda k: ()):
        def go(k):
            while pending[k] and pending[k][0][0] < time:
                _, p, d = pending[k].pop(0)
                need(k, p)
                c, o = place(k, p)
                copy(c, d, o).start()
            for p in wanted(k):
                need(k, p)

        by_role(go)

    def loop(lo, hi, f):
        lax.fori_loop(lo, hi, lambda i, _: (f(i), _)[1], 0)

    R = min(rows, 512)

    turns = {(k, m): plan.order(k, m) for k in plan.roles() for m in range(2)}

    def dots(m, t, groups=range(G), last=False):
        zo = z
        for k in plan.roles():
            zo = jnp.where(role == k, z + ahead * (turns[k, m][t] - k), zo)

        def tile(i):
            r = pl.ds(pl.multiple_of(i * R, R), R)
            p = pl.ds(pl.multiple_of(zo * plane, plane), plane)
            for j in groups:
                part = jnp.dot(PR[r, p], W[m * G + j, p, :], preferred_element_type=F32)
                if t > 0:
                    part = acc[j, r, :] + part
                if last:
                    v_out[r, pl.ds(j * width, width)] = part.astype(BF16)
                else:
                    acc[j, r, :] = part

        loop(0, rows // R, tile)

    barrier = pltpu.get_barrier_semaphore()
    for d in range(1, tp):
        pl.semaphore_signal(
            barrier, inc=1, device_id={"tp": (mt + d) % tp}, device_id_type=pl.DeviceIdType.MESH)

    def signal(sem, d):
        pl.semaphore_signal(
            sem, inc=1, device_id={"sp": partner[d]}, device_id_type=pl.DeviceIdType.MESH)

    signal(barrier, X)
    signal(barrier, Y)
    pl.when(up_ok)(lambda: signal(barrier, UP))
    pl.when(down_ok)(lambda: signal(barrier, DOWN))

    def columns(t):
        return PR.at[:, pl.ds(pl.multiple_of(t * wl, wl), wl)]

    own = [
        pltpu.make_async_copy(
            w.at[:, pl.ds(j * width, width)], piece(m * G + j, me), loc.at[m])
        for m, w in enumerate((wk, wv)) for j in range(G)
    ]
    rest = [
        pltpu.make_async_copy(src, dst, loc.at[2 + i])
        for i, (src, dst) in enumerate((
            (fresh, fr), (prompt.at[0], columns(mt)), (wq, wq_v), (lam, lam_v), (gain, gain_out)))
    ]

    def own_wait(m):
        whole = W.at[pl.ds(m * G, G), pl.ds(pl.multiple_of(me * depth, depth), depth), :]
        pltpu.make_async_copy(whole, whole, loc.at[m]).wait()

    for c in own[:G]:
        c.start()
    rest[0].start()
    for c in own[G:]:
        c.start()
    for c in rest[1:]:
        c.start()
    own_wait(0)

    @pl.when(up_ok & down_ok)
    def _():
        pl.semaphore_wait(barrier, 4 + tp - 1)

    @pl.when(outer)
    def _():
        pl.semaphore_wait(barrier, 3 + tp - 1)


    block_of = XR.shape[2]
    share = wl // depth
    mine = me // share == mt

    def features(chip):
        first_one = (chip * depth) % wl // block_of * block_of
        return pl.ds(pl.multiple_of(first_one, block_of), block_of)

    def x_sends():
        def to(i):
            chip, t = mt * share + (me + i // tp) % share, (mt + i) % tp

            @pl.when((chip != me) | (t != mt))
            def _():
                pltpu.make_async_remote_copy(
                    src_ref=fr.at[:, features(chip)], dst_ref=XR.at[me],
                    send_sem=x_send.at[0], recv_sem=x_recv.at[0],
                    device_id={"sp": chip, "tp": t}, device_id_type=pl.DeviceIdType.MESH,
                ).start()

        loop(0, n, to)

        @pl.when(mine)
        def _():
            XR[me] = fr[:, features(me)]

    def together(ref, send_sem, recv_sem):
        return pltpu.make_async_remote_copy(
            src_ref=ref, dst_ref=ref, send_sem=send_sem.at[0], recv_sem=recv_sem.at[0],
            device_id={"sp": partner[X]}, device_id_type=pl.DeviceIdType.MESH,
        )

    def x_wait(end):
        pl.when(mine)(lambda: end(together(XR.at[pl.ds(0, n - 1)], x_send, x_recv)))
        pl.when(jnp.logical_not(mine))(lambda: end(together(XR, x_send, x_recv)))

    q_all = together(QR.at[pl.ds(0, n - 1)], q_send, q_recv)

    def p_copy(d):
        return pltpu.make_async_remote_copy(
            src_ref=prompt.at[0], dst_ref=columns(mt),
            send_sem=p_send.at[d], recv_sem=p_recv.at[mt],
            device_id={"tp": (mt + d) % tp}, device_id_type=pl.DeviceIdType.MESH,
        )

    def p_wait(d):
        src = (mt + d) % tp
        return pltpu.make_async_remote_copy(
            src_ref=columns(src), dst_ref=columns(src),
            send_sem=p_send.at[d], recv_sem=p_recv.at[src],
            device_id={"tp": src}, device_id_type=pl.DeviceIdType.MESH,
        )

    advance(0.0001)
    signal(token.at[Y], Y)

    def relay_token(b):
        for turn, before, more, d in ((z == b, down_ok, up_ok, UP), (z == L - 1 - b, up_ok, down_ok, DOWN)):
            pl.when(turn & before)(lambda d=d: pl.semaphore_wait(token.at[d], 1))
            pl.when(turn & more)(lambda d=d: signal(token.at[d], d))

    rest[0].wait()
    own_wait(1)
    for d in range(1, tp):
        p_copy(d).start()


    def q_copy(d):
        dst = (me + d) % n
        return pltpu.make_async_remote_copy(
            src_ref=QS.at[dst], dst_ref=QR.at[me],
            send_sem=q_send.at[0], recv_sem=q_recv.at[0],
            device_id={"sp": dst}, device_id_type=pl.DeviceIdType.MESH,
        )

    def partial_queries():
        x_wait(lambda c: c.wait_recv())
        for j in range(n):
            XM[pl.ds(j, 1), :] = XR[j].astype(F32)
        chosen = XM[...].astype(BF16)
        if block_of > depth:
            pick = (
                lax.broadcasted_iota(jnp.int32, (block_of, depth), 0)
                == me * depth % block_of + lax.broadcasted_iota(jnp.int32, (block_of, depth), 1)
            )
            chosen = jnp.dot(
                chosen, jnp.where(pick, 1.0, 0.0).astype(BF16), preferred_element_type=F32).astype(BF16)
        rest[2].wait()
        partial = jnp.dot(chosen, wq_v[...], preferred_element_type=F32)
        for j in range(n):
            QS[j] = partial[j:j + 1, :]
        QR[me] = QS[me]
        loop(1, n, lambda d: q_copy(d).start())

    hp = max(heads, 8)
    pad = 2 * hp

    def build_query():
        qcos, qsin = table(jnp.full((8, LANES), rows, F32))
        q_all.wait_recv()
        total = QR[0]
        for j in range(1, n):
            total = total + QR[j]
        total = jnp.broadcast_to(total, (8, cols))
        query = jnp.concatenate(
            [rotated(total[:, i:i + LANES], qcos, qsin) for i in range(0, cols, LANES)], axis=1)
        query = jnp.broadcast_to(query[:1], (pad, cols))
        row = lax.broadcasted_iota(jnp.int32, (pad, cols), 0)
        keep = 2 * (row % hp) + row // hp == lax.broadcasted_iota(jnp.int32, (pad, cols), 1) // MAP_DIM
        qs[...] = jnp.where(keep, query, 0.0).astype(BF16)

    def angles(i):
        position = (i * 64 + lax.broadcasted_iota(jnp.int32, (64, LANES), 0)).astype(F32)
        r = pl.ds(pl.multiple_of(i * 64, 64), 64)
        ct[r, :], st[r, :] = table(position)

    RR = min(rows, 256)

    def rotate_rows(i):
        r = pl.ds(pl.multiple_of(i * RR, RR), RR)
        cosine, sine = ct[r, :], st[r, :]
        for i in range(0, cols, LANES):
            tile = acc[i // width, r, pl.ds(i % width, LANES)]
            k_out[r, pl.ds(i, LANES)] = rotated(tile, cosine, sine).astype(BF16)

    def weigh():
        scores = lax.dot_general(
            qs[...], k_out[...], (((1,), (1,)), ((), ())), preferred_element_type=F32) * MAP_DIM ** -0.5
        weights = jnp.exp(scores - jnp.max(scores, axis=-1, keepdims=True))
        weights = weights / jnp.sum(weights, axis=-1, keepdims=True)
        rest[3].wait()
        here = (lax.broadcasted_iota(jnp.int32, (hp, heads), 0)
                == lax.broadcasted_iota(jnp.int32, (hp, heads), 1))
        scale = jnp.sum(jnp.where(here, lam_v[...], 0.0), axis=-1, keepdims=True)
        mix = weights[:hp] - scale * weights[hp:]
        high = mix.astype(BF16)
        left = mix - high.astype(F32)
        mid = left.astype(BF16)
        low = (left - mid.astype(F32)).astype(BF16)
        mix_out[...] = jnp.concatenate([high, mid, low], axis=0)

    def when_ready(m, t, groups):
        return max(plan.ready(k, m, turns[k, m][t], groups) for k in plan.roles())

    def prompt_whole():
        rest[1].wait()
        for d in range(1, tp):
            p_wait(d).wait_recv()

    def first_token():
        pl.semaphore_wait(token.at[Y], 1)
        signal(token.at[X], X)

    def second_token():
        pl.semaphore_wait(token.at[X], 1)
        relay_token(0)

    def turn_rows(i):
        loop(i * (rows // RR) // 2, (i + 1) * (rows // RR) // 2, rotate_rows)

    none = lambda k: ()
    work = [
        (TOK0, first_token, none), (TOK1, second_token, none),
        *((TOK1 + 0.9 * b, functools.partial(relay_token, b), none) for b in range(1, L)),
    ]
    sent_x = TOK1 + 0.9 * L
    work.append((sent_x, x_sends, none))
    work.append((sent_x + 9, partial_queries, none))
    work.append((sent_x + 4, lambda: loop(0, rows // 64, angles), none))
    keys_at = 0
    for m in range(2):
        for t in range(L):
            last = m == 1 and t == L - 1
            when = when_ready(m, t, range(G)) + 0.1
            if m == 0 and t == 0:
                work.append((when, prompt_whole, none))
            if m == 1 and t == 0:
                when = max(when, keys_at + 2.5)
            if m == 0:
                keys_at = max(keys_at, when)
            work.append((
                when + 0.001 * t, functools.partial(dots, m, t, last=last),
                lambda k, m=m, t=t: plan.pieces(m, turns[k, m][t], range(G))))
    work.append((keys_at + 0.1, lambda: turn_rows(0), none))
    work.append((keys_at + 1.3, lambda: turn_rows(1), none))
    answer = max(sent_x + 9 + 12, keys_at + 2.4)
    work.append((answer, build_query, none))
    work.append((answer + 0.5, weigh, none))
    for time, act, wanted in sorted(work, key=lambda item: item[0]):
        advance(time, wanted)
        act()
    assert not any(pending.values())
    rest[4].wait()
    x_wait(lambda c: c.wait_send())
    q_all.wait_send()
    for d in range(1, tp):
        p_copy(d).wait_send()

    def sent(d, pieces):
        all_of = W.at[:, pl.ds(0, pieces * depth // G), :]
        pltpu.make_async_remote_copy(
            src_ref=all_of, dst_ref=all_of, send_sem=w_send.at[d], recv_sem=w_recv.at[0],
            device_id={"sp": partner[X]}, device_id_type=pl.DeviceIdType.MESH,
        ).wait_send()

    def settle(k):
        for d in range(4):
            pieces = sum(link == d for _, link in plan.start[k])
            if pieces:
                sent(d, pieces // 2)

    by_role(settle)


def read(keys, values, mix, gain, k_out, v_out, read_out, sem):
    hp = mix.shape[0] // 3
    heads = read_out.shape[1]
    k_copy = pltpu.make_async_copy(keys, k_out.at[0], sem.at[0])
    v_copy = pltpu.make_async_copy(values, v_out.at[0], sem.at[1])
    v_copy.start()
    k_copy.start()
    mixed = jnp.dot(mix[...], values[...], preferred_element_type=F32)
    mixed = mixed[:hp] + mixed[hp:2 * hp] + mixed[2 * hp:]
    diff = jnp.concatenate(
        [mixed[h:h + 1, h * VAL_DIM:(h + 1) * VAL_DIM] for h in range(heads)], axis=0)
    normed = diff * lax.rsqrt(jnp.mean(diff * diff, axis=-1, keepdims=True) + norm_eps)
    read_out[0] = (normed * gain[...]).astype(BF16)
    v_copy.wait()
    k_copy.wait()


def body(n, tp, prompt, new_input, w_query, w_key, w_value, lam, out_gain):
    seqs, rows, wl = prompt.shape
    depth, cols = w_key.shape
    heads = lam.shape[0]
    G = groups(cols)
    hp = max(heads, 8)
    operands = [
        pltpu.with_memory_space_constraint(a, pltpu.HBM)
        for a in (prompt, new_input, w_query, w_key, w_value, lam[None, :], out_gain[None, :])
    ]
    any_ = pl.BlockSpec(memory_space=pl.ANY)
    hbm = pl.BlockSpec(memory_space=pltpu.HBM)
    vmem = pl.BlockSpec(memory_space=pltpu.VMEM)
    dma = pltpu.SemaphoreType.DMA
    keys, values, mix, gain = pl.pallas_call(
        functools.partial(kernel, n, tp, G, heads),
        out_shape=(
            pltpu.VMEM((rows, cols), BF16),
            pltpu.VMEM((rows, cols), BF16),
            pltpu.VMEM((3 * hp, rows), BF16),
            pltpu.VMEM((1, VAL_DIM), F32),
        ),
        in_specs=[hbm] * 7,
        out_specs=(vmem, vmem, vmem, vmem),
        scratch_shapes=[
            pltpu.VMEM((2 * G, n * depth, cols // G), BF16),
            pltpu.VMEM((rows, tp * wl), BF16),
            pltpu.VMEM((G, rows, cols // G), F32),
            pltpu.VMEM((1, wl), BF16),
            pltpu.VMEM((n, 1, max(depth, LANES)), BF16),
            pltpu.VMEM((n, max(depth, LANES)), F32),
            pltpu.VMEM((depth, cols), BF16),
            pltpu.VMEM((n, 1, cols), F32),
            pltpu.VMEM((n, 1, cols), F32),
            pltpu.VMEM((rows, LANES), F32),
            pltpu.VMEM((rows, LANES), F32),
            pltpu.VMEM((2 * hp, cols), BF16),
            pltpu.VMEM((1, heads), F32),
            dma((2 * G * n,)), dma((4,)), dma((tp,)), dma((tp,)), dma((1,)), dma((1,)),
            dma((1,)), dma((1,)), dma((7,)),
            pltpu.SemaphoreType.REGULAR((4,)),
        ],
        compiler_params=pltpu.CompilerParams(
            collective_id=0, has_side_effects=True, vmem_limit_bytes=44 * 1024 * 1024),
        name="prefill",
    )(*operands)
    return pl.pallas_call(
        read,
        out_shape=(
            jax.ShapeDtypeStruct((seqs, rows, cols), BF16),
            jax.ShapeDtypeStruct((seqs, rows, cols), BF16),
            jax.ShapeDtypeStruct((seqs, heads, VAL_DIM), BF16),
        ),
        in_specs=[vmem] * 4,
        out_specs=(any_, any_, vmem),
        scratch_shapes=[dma((2,))],
        compiler_params=pltpu.CompilerParams(vmem_limit_bytes=24 * 1024 * 1024),
        name="read",
    )(keys, values, mix, gain)


def solution(mesh):
    in_specs = (
        P("sp", None, "tp"), P("sp", "tp"), P("sp", "tp"), P("sp", "tp"), P("sp", "tp"), P("tp"), P(),
    )
    out_specs = (P("sp", None, "tp"), P("sp", None, "tp"), P("sp", "tp", None))
    return jax.shard_map(
        functools.partial(body, mesh.shape["sp"], mesh.shape["tp"]),
        mesh=mesh, in_specs=in_specs, out_specs=out_specs, check_vma=False)
```

```python
import functools
import heapq
import math

import jax
import jax.numpy as jnp
from jax import lax
from jax.experimental import pallas as pl
from jax.experimental.pallas import tpu as pltpu
from jax.sharding import PartitionSpec as P

MAP_DIM = 64
VAL_DIM = 128
LANES = 128
rope_base = 500000.0
norm_eps = 1e-05

X, Y, UP, DOWN = 0, 1, 2, 3
LAG, LEAD = 0.9, 3.0
TOKC, TOK0, TOK1 = 1.0, 2.5, 4.0
F32, BF16 = jnp.float32, jnp.bfloat16


def inverse_freq(shape):
    lane = lax.broadcasted_iota(jnp.int32, shape, 1) % (MAP_DIM // 2)
    return jnp.exp(lane.astype(F32) * (-2.0 / MAP_DIM * math.log(rope_base)))


def table(position):
    angle = position * inverse_freq(position.shape)
    lane = lax.broadcasted_iota(jnp.int32, angle.shape, 1) % MAP_DIM
    sine = jnp.sin(angle)
    return jnp.cos(angle), jnp.where(lane < MAP_DIM // 2, -sine, sine)


def rotated(tile, cosine, sine):
    half = MAP_DIM // 2
    lane = lax.broadcasted_iota(jnp.int32, tile.shape, 1) % MAP_DIM
    other = jnp.where(lane < half, pltpu.roll(tile, LANES - half, 1), pltpu.roll(tile, half, 1))
    return tile * cosine + other * sine


def groups(cols):
    return max(g for g in (4, 2, 1) if cols % (g * LANES) == 0)


class Plan:
    def __init__(self, L, G):
        self.L, self.G = L, G
        self.first = [X if j < (G + 1) // 2 else Y for j in range(G)]
        self.wide = [G >= 4 and j % 2 == 1 for j in range(G)]
        self.arrival = [{} for _ in range(L)]
        self.start = [{} for _ in range(L)]
        waiting = {(z, d): [] for z in range(L) for d in range(4)}
        free = dict.fromkeys(waiting, 0.0)
        events, count = [], 0

        def post(time, what):
            nonlocal count
            count += 1
            heapq.heappush(events, (time, count, what))

        def begin(z, d, time):
            if waiting[z, d] and free[z, d] <= time:
                piece = heapq.heappop(waiting[z, d])[-1]
                self.start[z][piece, d] = time
                free[z, d] = time + 1
                post(time + 1, (z, d, None))
                post(time + 1 + LAG, (*self.beyond(z, piece, d)[:1], None, self.beyond(z, piece, d)[1]))

        for z in range(L):
            for m in range(2):
                for j in range(G):
                    post(0.0, (z, None, (m, j, z, 0, 0)))
        while events:
            time, _, (z, d, piece) = heapq.heappop(events)
            if d is not None:
                begin(z, d, time)
                continue
            assert piece not in self.arrival[z]
            self.arrival[z][piece] = time
            for d in self.links(z, piece):
                count += 1
                goes_on = bool(self.links(*self.beyond(z, piece, d)))
                heapq.heappush(waiting[z, d], (self.rank(z, piece, d), count, piece))
            for d in range(4):
                begin(z, d, time)
        self.end = max(max(a.values()) for a in self.arrival)

    def rank(self, z, piece, d):
        m, j, zo, dy, dx = piece
        there, seen = self.beyond(z, piece, d)
        relayed = any(link in (X, Y) for link in self.links(there, seen))
        return m, not relayed

    def outer(self, zo):
        return zo in (0, self.L - 1)

    def links(self, z, piece):
        m, j, zo, dy, dx = piece
        along = [d for d, step in ((UP, 1), (DOWN, -1))
                 if 0 <= z + step < self.L and (z == zo or (step > 0) == (z > zo))]
        second = [X + Y - self.first[j]]
        if (dy, dx) == (0, 0):
            if z == zo or not self.outer(zo):
                return along + [X, Y]
            return along + second * (not self.wide[j])
        if (dx if self.first[j] == X else dy) and not (dx and dy):
            along = along * self.outer(zo)
            return along + second * (z == zo or not self.outer(zo) or not self.wide[j])
        return along * (self.outer(zo) and self.wide[j])

    def beyond(self, z, piece, d):
        m, j, zo, dy, dx = piece
        return z + (d == UP) - (d == DOWN), (m, j, zo, dy ^ (d == Y), dx ^ (d == X))

    def roles(self):
        return range((self.L + 1) // 2)

    def sends(self, k):
        own = ((max(self.arrival[k][p], t - LEAD), t, p, d) for (p, d), t in self.start[k].items())
        return [(when, p, d) for when, _, p, d in sorted(own)]

    def pieces(self, m, zo, groups, sides=(0, 1)):
        return [(m, j, zo, dy, dx) for j in groups for dy in sides for dx in range(2)]

    def ready(self, k, m, zo, groups, sides=(0, 1)):
        return max(self.arrival[k][p] for p in self.pieces(m, zo, groups, sides))

    def order(self, k, m):
        everything = range(self.G)
        return sorted(range(self.L), key=lambda zo: (zo != k, self.ready(k, m, zo, everything)))


def rows_of(zo, y, depth):
    if 2 * depth % LANES:
        return pl.ds(pl.multiple_of(zo * 4 * depth, 4 * depth), 4 * depth)
    return pl.ds(pl.multiple_of((zo * 4 + y * 2) * depth, 2 * depth), 2 * depth)


def ending(plan, z):
    L, m = plan.L, 1
    role = jnp.minimum(z, L - 1 - z)
    ahead = jnp.where(z <= L - 1 - z, 1, -1)
    zo, ready = z, {j: 0.0 for j in range(plan.G)}
    for k in plan.roles():
        final = plan.order(k, m)[-1]
        zo = jnp.where(role == k, z + ahead * (final - k), zo)
        for j in ready:
            ready[j] = max(ready[j], plan.ready(k, m, final, [j]))
    return role, ahead, zo, [j for j in ready if ready[j] > max(ready.values()) - 0.5]


def kernel(
    n, tp, G, heads, prompt, fresh, wq, wk, wv, lam, gain,
    k_out, v_out, mix_out, gain_out, W, PR, acc,
    fr, XR, XM, wq_v, QS, QR, ct, st, qs, lam_v,
    w_recv, w_send, p_recv, p_send, x_recv, x_send, q_recv, q_send, loc, token,
):
    _, rows, wl = prompt.shape
    depth, cols = wk.shape
    width = cols // G
    L = n // 4
    plane = 4 * depth
    me, mt = lax.axis_index("sp"), lax.axis_index("tp")
    z, y, x = me // 4, (me // 2) % 2, me % 2
    yf, xf = 1 - y, 1 - x
    up_ok, down_ok = z + 1 < L, z > 0
    outer = jnp.logical_not(up_ok & down_ok)

    plan = Plan(L, G)
    role, ahead, last_plane, late = ending(plan, z)

    def at(zo, yo, xo):
        return zo * 4 + yo * 2 + xo

    partner = {X: at(z, y, xf), Y: at(z, yf, x), UP: me + 4, DOWN: me - 4}

    def piece(c, o):
        return W.at[c, pl.ds(pl.multiple_of(o * depth, depth), depth), :]

    target = {X: partner[X], Y: partner[Y], UP: me + 4 * ahead, DOWN: me - 4 * ahead}

    def place(k, p):
        m, j, zo, dy, dx = p
        return m * G + j, at(z + ahead * (zo - k), yf if dy else y, xf if dx else x)

    def copy(c, d, o):
        return pltpu.make_async_remote_copy(
            src_ref=piece(c, o), dst_ref=piece(c, o),
            send_sem=w_send.at[d], recv_sem=w_recv.at[c * n + o],
            device_id={"sp": target[d]}, device_id_type=pl.DeviceIdType.MESH,
        )

    def by_role(f):
        for k in plan.roles():
            pl.when(role == k)(functools.partial(f, k))

    pending = {k: plan.sends(k) for k in plan.roles()}
    arrived = {k: set(plan.pieces(0, k, range(0))) for k in plan.roles()}

    def need(k, p):
        if p[2:] != (k, 0, 0) and p not in arrived[k]:
            arrived[k].add(p)
            c, o = place(k, p)
            copy(c, X, o).wait_recv()

    def advance(time, wanted=lambda k: ()):
        def go(k):
            while pending[k] and pending[k][0][0] < time:
                _, p, d = pending[k].pop(0)
                need(k, p)
                c, o = place(k, p)
                copy(c, d, o).start()
            for p in wanted(k):
                need(k, p)

        by_role(go)

    def loop(lo, hi, f):
        lax.fori_loop(lo, hi, lambda i, _: (f(i), _)[1], 0)

    turns = {(k, m): plan.order(k, m) for k in plan.roles() for m in range(2)}

    def dots(m, t, groups=range(G), sides=(0, 1), last=False):
        zo = z
        for k in plan.roles():
            zo = jnp.where(role == k, z + ahead * (turns[k, m][t] - k), zo)

        R = rows // len(sides)

        def tile(i):
            r = pl.ds(pl.multiple_of(i * R, R), R)
            if len(sides) == 2:
                p = pl.ds(pl.multiple_of(zo * plane, plane), plane)
            else:
                p = rows_of(zo, yf if sides[0] else y, depth)
            for j in groups:
                part = jnp.dot(PR[r, p], W[m * G + j, p, :], preferred_element_type=F32)
                if t > 0 or sides == (1,):
                    part = acc[j, r, :] + part
                if last:
                    v_out[r, pl.ds(j * width, width)] = part.astype(BF16)
                else:
                    acc[j, r, :] = part

        loop(0, rows // R, tile)

    barrier = pltpu.get_barrier_semaphore()

    def cores(which, sem):
        for t in range(tp):
            @pl.when(t > mt if which > 0 else t < mt)
            def _(t=t):
                pl.semaphore_signal(sem, inc=1, device_id={"tp": t}, device_id_type=pl.DeviceIdType.MESH)

    cores(1, barrier)

    def signal(sem, d):
        pl.semaphore_signal(
            sem, inc=1, device_id={"sp": partner[d]}, device_id_type=pl.DeviceIdType.MESH)

    signal(barrier, X)
    signal(barrier, Y)
    pl.when(up_ok)(lambda: signal(barrier, UP))
    pl.when(down_ok)(lambda: signal(barrier, DOWN))

    def columns(t):
        return PR.at[:, pl.ds(pl.multiple_of(t * wl, wl), wl)]

    own = [
        pltpu.make_async_copy(
            w.at[:, pl.ds(j * width, width)], piece(m * G + j, me), loc.at[m])
        for m, w in enumerate((wk, wv)) for j in range(G)
    ]
    rest = [
        pltpu.make_async_copy(src, dst, loc.at[2 + i])
        for i, (src, dst) in enumerate((
            (fresh, fr), (prompt.at[0], columns(mt)), (wq, wq_v), (lam, lam_v), (gain, gain_out)))
    ]

    def own_wait(m):
        whole = W.at[pl.ds(m * G, G), pl.ds(pl.multiple_of(me * depth, depth), depth), :]
        pltpu.make_async_copy(whole, whole, loc.at[m]).wait()

    for c in own[:G]:
        c.start()
    rest[0].start()
    for c in own[G:]:
        c.start()
    for c in rest[1:]:
        c.start()
    own_wait(0)

    pl.semaphore_wait(barrier, 2 + up_ok.astype(jnp.int32) + down_ok.astype(jnp.int32) + mt)

    block_of = XR.shape[2]
    share = wl // depth
    mine = me // share == mt

    def features(chip):
        first_one = (chip * depth) % wl // block_of * block_of
        return pl.ds(pl.multiple_of(first_one, block_of), block_of)

    def x_sends():
        def to(i):
            chip, t = mt * share + (me + i // tp) % share, (mt + i) % tp

            @pl.when((chip != me) | (t != mt))
            def _():
                pltpu.make_async_remote_copy(
                    src_ref=fr.at[:, features(chip)], dst_ref=XR.at[me],
                    send_sem=x_send.at[0], recv_sem=x_recv.at[0],
                    device_id={"sp": chip, "tp": t}, device_id_type=pl.DeviceIdType.MESH,
                ).start()

        loop(0, n, to)

        @pl.when(mine)
        def _():
            XR[me] = fr[:, features(me)]

    def together(ref, send_sem, recv_sem):
        return pltpu.make_async_remote_copy(
            src_ref=ref, dst_ref=ref, send_sem=send_sem.at[0], recv_sem=recv_sem.at[0],
            device_id={"sp": partner[X]}, device_id_type=pl.DeviceIdType.MESH,
        )

    def x_wait(end):
        pl.when(mine)(lambda: end(together(XR.at[pl.ds(0, n - 1)], x_send, x_recv)))
        pl.when(jnp.logical_not(mine))(lambda: end(together(XR, x_send, x_recv)))

    q_all = together(QR.at[pl.ds(0, n - 1)], q_send, q_recv)

    def p_copy(d):
        return pltpu.make_async_remote_copy(
            src_ref=prompt.at[0], dst_ref=columns(mt),
            send_sem=p_send.at[d], recv_sem=p_recv.at[mt],
            device_id={"tp": (mt + d) % tp}, device_id_type=pl.DeviceIdType.MESH,
        )

    def p_wait(d):
        src = (mt + d) % tp
        return pltpu.make_async_remote_copy(
            src_ref=columns(src), dst_ref=columns(src),
            send_sem=p_send.at[d], recv_sem=p_recv.at[src],
            device_id={"tp": src}, device_id_type=pl.DeviceIdType.MESH,
        )

    advance(0.0001)
    cores(-1, token.at[4])

    def relay_token(b):
        for turn, before, more, d in ((z == b, down_ok, up_ok, UP), (z == L - 1 - b, up_ok, down_ok, DOWN)):
            pl.when(turn & before)(lambda d=d: pl.semaphore_wait(token.at[d], 1))
            pl.when(turn & more)(lambda d=d: signal(token.at[d], d))

    rest[0].wait()
    own_wait(1)


    def q_copy(d):
        dst = (me + d) % n
        return pltpu.make_async_remote_copy(
            src_ref=QS.at[dst], dst_ref=QR.at[me],
            send_sem=q_send.at[0], recv_sem=q_recv.at[0],
            device_id={"sp": dst}, device_id_type=pl.DeviceIdType.MESH,
        )

    def partial_queries():
        x_wait(lambda c: c.wait_recv())
        for j in range(n):
            XM[pl.ds(j, 1), :] = XR[j].astype(F32)
        chosen = XM[...].astype(BF16)
        if block_of > depth:
            pick = (
                lax.broadcasted_iota(jnp.int32, (block_of, depth), 0)
                == me * depth % block_of + lax.broadcasted_iota(jnp.int32, (block_of, depth), 1)
            )
            chosen = jnp.dot(
                chosen, jnp.where(pick, 1.0, 0.0).astype(BF16), preferred_element_type=F32).astype(BF16)
        rest[2].wait()
        partial = jnp.dot(chosen, wq_v[...], preferred_element_type=F32)
        for j in range(n):
            QS[j] = partial[j:j + 1, :]
        QR[me] = QS[me]
        loop(1, n, lambda d: q_copy(d).start())

    hp = max(heads, 8)
    pad = 2 * hp

    def build_query():
        qcos, qsin = table(jnp.full((8, LANES), rows, F32))
        q_all.wait_recv()
        total = QR[0]
        for j in range(1, n):
            total = total + QR[j]
        total = jnp.broadcast_to(total, (8, cols))
        query = jnp.concatenate(
            [rotated(total[:, i:i + LANES], qcos, qsin) for i in range(0, cols, LANES)], axis=1)
        query = jnp.broadcast_to(query[:1], (pad, cols))
        row = lax.broadcasted_iota(jnp.int32, (pad, cols), 0)
        keep = 2 * (row % hp) + row // hp == lax.broadcasted_iota(jnp.int32, (pad, cols), 1) // MAP_DIM
        qs[...] = jnp.where(keep, query, 0.0).astype(BF16)

    def angles(i):
        position = (i * 64 + lax.broadcasted_iota(jnp.int32, (64, LANES), 0)).astype(F32)
        r = pl.ds(pl.multiple_of(i * 64, 64), 64)
        ct[r, :], st[r, :] = table(position)

    RR = min(rows, 256)

    def rotate_rows(i):
        r = pl.ds(pl.multiple_of(i * RR, RR), RR)
        cosine, sine = ct[r, :], st[r, :]
        for i in range(0, cols, LANES):
            tile = acc[i // width, r, pl.ds(i % width, LANES)]
            k_out[r, pl.ds(i, LANES)] = rotated(tile, cosine, sine).astype(BF16)

    def weigh():
        scores = lax.dot_general(
            qs[...], k_out[...], (((1,), (1,)), ((), ())), preferred_element_type=F32) * MAP_DIM ** -0.5
        weights = jnp.exp(scores - jnp.max(scores, axis=-1, keepdims=True))
        weights = weights / jnp.sum(weights, axis=-1, keepdims=True)
        rest[3].wait()
        here = (lax.broadcasted_iota(jnp.int32, (hp, heads), 0)
                == lax.broadcasted_iota(jnp.int32, (hp, heads), 1))
        scale = jnp.sum(jnp.where(here, lam_v[...], 0.0), axis=-1, keepdims=True)
        mix = weights[:hp] - scale * weights[hp:]
        high = mix.astype(BF16)
        left = mix - high.astype(F32)
        mid = left.astype(BF16)
        low = (left - mid.astype(F32)).astype(BF16)
        mix_out[...] = jnp.concatenate([high, mid, low], axis=0)

    def when_ready(m, t, groups, sides=(0, 1)):
        return max(plan.ready(k, m, turns[k, m][t], groups, sides) for k in plan.roles())

    def add_dots(when, m, t, groups=range(G), sides=(0, 1), last=False):
        def wanted(k):
            return plan.pieces(m, turns[k, m][t], groups, sides)

        work.append((when, functools.partial(dots, m, t, groups, sides, last), wanted))

    def prompt_whole():
        rest[1].wait()
        for d in range(1, tp):
            p_wait(d).wait_recv()

    def all_cores():
        pl.when(mt < tp - 1)(lambda: pl.semaphore_wait(token.at[4], tp - 1 - mt))
        signal(token.at[Y], Y)
        for d in range(1, tp):
            p_copy(d).start()

    def first_token():
        pl.semaphore_wait(token.at[Y], 1)
        signal(token.at[X], X)

    def second_token():
        pl.semaphore_wait(token.at[X], 1)
        relay_token(0)

    def turn_rows(i):
        loop(i * (rows // RR) // 2, (i + 1) * (rows // RR) // 2, rotate_rows)

    none = lambda k: ()
    work = [
        (TOKC, all_cores, none), (TOK0, first_token, none), (TOK1, second_token, none),
        *((TOK1 + 0.9 * b, functools.partial(relay_token, b), none) for b in range(1, L)),
    ]
    sent_x = TOK1 + 0.9 * L
    work.append((sent_x, x_sends, none))
    work.append((sent_x + 9, partial_queries, none))
    work.append((sent_x + 4, lambda: loop(0, rows // 64, angles), none))
    keys_at = 0
    for m in range(2):
        for t in range(L):
            when = when_ready(m, t, range(G)) + 0.1 + 0.001 * t
            if m == 0:
                keys_at = max(keys_at, when)
            if (m, t) == (0, 0):
                work.append((when - 0.01, prompt_whole, none))
            if (m, t) == (1, 0):
                when = max(when, keys_at + 2.5)
            if m == 0 or t < max(L - 2, 1):
                add_dots(when, m, t)
                continue
            last, after = t == L - 1, 0
            for sides in ([(0,), (1,)] if 2 * depth % LANES == 0 else [(0, 1)]):
                ready = {j: when_ready(m, t, [j], sides) for j in range(G)}
                if not last:
                    parts = [list(range(G))]
                elif sides == (0,):
                    edge = max(ready.values()) - 3
                    parts = [[j for j in ready if ready[j] < edge], [j for j in ready if ready[j] >= edge]]
                else:
                    parts = [[j for j in ready if j not in late]]
                for some in parts:
                    if some:
                        after = max(after, max(ready[j] for j in some)) + 0.02
                        add_dots(after + 0.01 * t, m, t, some, sides, last and 1 in sides)
    work.append((keys_at + 0.1, lambda: turn_rows(0), none))
    work.append((keys_at + 1.3, lambda: turn_rows(1), none))
    answer = max(sent_x + 9 + 12, keys_at + 2.4)
    work.append((answer, build_query, none))
    work.append((answer + 0.5, weigh, none))
    for time, act, wanted in sorted(work, key=lambda item: item[0]):
        advance(time, wanted)
        act()
    advance(2 * plan.end, lambda k: plan.pieces(1, turns[k, 1][L - 1], late))
    rest[4].wait()
    x_wait(lambda c: c.wait_send())
    q_all.wait_send()
    for d in range(1, tp):
        p_copy(d).wait_send()

    def sent(d, pieces):
        all_of = W.at[:, pl.ds(0, pieces * depth // G), :]
        pltpu.make_async_remote_copy(
            src_ref=all_of, dst_ref=all_of, send_sem=w_send.at[d], recv_sem=w_recv.at[0],
            device_id={"sp": partner[X]}, device_id_type=pl.DeviceIdType.MESH,
        ).wait_send()

    def settle(k):
        for d in range(4):
            pieces = sum(link == d for _, link in plan.start[k])
            if pieces:
                sent(d, pieces // 2)

    by_role(settle)


def read(n, G, keys, values, mix, gain, W, PR, acc, k_out, v_out, read_out, fresh, sem):
    hp = mix.shape[0] // 3
    heads = read_out.shape[1]
    depth, width = W.shape[1] // n, W.shape[2]
    me = lax.axis_index("sp")
    _, _, zo, late = ending(Plan(n // 4, G), me // 4)
    k_copy = pltpu.make_async_copy(keys, k_out.at[0], sem.at[0])
    k_copy.start()

    def columns(j):
        return pl.ds(j * width, width)

    source = [fresh if j in late else values for j in range(G)]
    v_copies = [
        pltpu.make_async_copy(source[j].at[:, columns(j)], v_out.at[0, :, columns(j)], sem.at[1 + j])
        for j in range(G)
    ]
    for j in range(G):
        if j not in late:
            v_copies[j].start()
    p = rows_of(zo, 1 - (me // 2) % 2, depth)
    for j in late:
        part = acc[j] + jnp.dot(PR[:, p], W[G + j, p, :], preferred_element_type=F32)
        fresh[:, columns(j)] = part.astype(BF16)
        v_copies[j].start()
    mixed = jnp.concatenate(
        [jnp.dot(mix[...], source[j][:, columns(j)], preferred_element_type=F32) for j in range(G)], axis=1)
    mixed = mixed[:hp] + mixed[hp:2 * hp] + mixed[2 * hp:]
    diff = jnp.concatenate(
        [mixed[h:h + 1, h * VAL_DIM:(h + 1) * VAL_DIM] for h in range(heads)], axis=0)
    normed = diff * lax.rsqrt(jnp.mean(diff * diff, axis=-1, keepdims=True) + norm_eps)
    read_out[0] = (normed * gain[...]).astype(BF16)
    for c in v_copies:
        c.wait()
    k_copy.wait()


def body(n, tp, prompt, new_input, w_query, w_key, w_value, lam, out_gain):
    seqs, rows, wl = prompt.shape
    depth, cols = w_key.shape
    heads = lam.shape[0]
    G = groups(cols)
    hp = max(heads, 8)
    operands = [
        pltpu.with_memory_space_constraint(a, pltpu.HBM)
        for a in (prompt, new_input, w_query, w_key, w_value, lam[None, :], out_gain[None, :])
    ]
    any_ = pl.BlockSpec(memory_space=pl.ANY)
    hbm = pl.BlockSpec(memory_space=pltpu.HBM)
    vmem = pl.BlockSpec(memory_space=pltpu.VMEM)
    dma = pltpu.SemaphoreType.DMA
    keys, values, *passed = pl.pallas_call(
        functools.partial(kernel, n, tp, G, heads),
        out_shape=(
            pltpu.VMEM((rows, cols), BF16),
            pltpu.VMEM((rows, cols), BF16),
            pltpu.VMEM((3 * hp, rows), BF16),
            pltpu.VMEM((1, VAL_DIM), F32),
            pltpu.VMEM((2 * G, n * depth, cols // G), BF16),
            pltpu.VMEM((rows, tp * wl), BF16),
            pltpu.VMEM((G, rows, cols // G), F32),
        ),
        in_specs=[hbm] * 7,
        out_specs=(vmem,) * 7,
        scratch_shapes=[
            pltpu.VMEM((1, wl), BF16),
            pltpu.VMEM((n, 1, max(depth, LANES)), BF16),
            pltpu.VMEM((n, max(depth, LANES)), F32),
            pltpu.VMEM((depth, cols), BF16),
            pltpu.VMEM((n, 1, cols), F32),
            pltpu.VMEM((n, 1, cols), F32),
            pltpu.VMEM((rows, LANES), F32),
            pltpu.VMEM((rows, LANES), F32),
            pltpu.VMEM((2 * hp, cols), BF16),
            pltpu.VMEM((1, heads), F32),
            dma((2 * G * n,)), dma((4,)), dma((tp,)), dma((tp,)), dma((1,)), dma((1,)),
            dma((1,)), dma((1,)), dma((7,)),
            pltpu.SemaphoreType.REGULAR((5,)),
        ],
        compiler_params=pltpu.CompilerParams(
            collective_id=0, has_side_effects=True, vmem_limit_bytes=20 * 1024 * 1024),
        name="prefill",
    )(*operands)
    return pl.pallas_call(
        functools.partial(read, n, G),
        out_shape=(
            jax.ShapeDtypeStruct((seqs, rows, cols), BF16),
            jax.ShapeDtypeStruct((seqs, rows, cols), BF16),
            jax.ShapeDtypeStruct((seqs, heads, VAL_DIM), BF16),
        ),
        in_specs=[vmem] * 7,
        out_specs=(any_, any_, vmem),
        scratch_shapes=[pltpu.VMEM((rows, cols), BF16), dma((1 + G,))],
        compiler_params=pltpu.CompilerParams(vmem_limit_bytes=24 * 1024 * 1024),
        name="read",
    )(keys, values, *passed)


def solution(mesh):
    in_specs = (
        P("sp", None, "tp"), P("sp", "tp"), P("sp", "tp"), P("sp", "tp"), P("sp", "tp"), P("tp"), P(),
    )
    out_specs = (P("sp", None, "tp"), P("sp", None, "tp"), P("sp", "tp", None))
    return jax.shard_map(
        functools.partial(body, mesh.shape["sp"], mesh.shape["tp"]),
        mesh=mesh, in_specs=in_specs, out_specs=out_specs, check_vma=False)
```

```python
import functools
import heapq
import math

import jax
import jax.numpy as jnp
from jax import lax
from jax.experimental import pallas as pl
from jax.experimental.pallas import tpu as pltpu
from jax.sharding import PartitionSpec as P

MAP_DIM = 64
VAL_DIM = 128
LANES = 128
rope_base = 500000.0
norm_eps = 1e-05

X, Y, UP, DOWN = 0, 1, 2, 3
LAG, LEAD = 0.9, 2.0
TOKC, TOK0, TOK1 = 1.0, 2.5, 4.0
F32, BF16 = jnp.float32, jnp.bfloat16


def inverse_freq(shape):
    lane = lax.broadcasted_iota(jnp.int32, shape, 1) % (MAP_DIM // 2)
    return jnp.exp(lane.astype(F32) * (-2.0 / MAP_DIM * math.log(rope_base)))


def table(position):
    angle = position * inverse_freq(position.shape)
    lane = lax.broadcasted_iota(jnp.int32, angle.shape, 1) % MAP_DIM
    sine = jnp.sin(angle)
    return jnp.cos(angle), jnp.where(lane < MAP_DIM // 2, -sine, sine)


def rotated(tile, cosine, sine):
    half = MAP_DIM // 2
    lane = lax.broadcasted_iota(jnp.int32, tile.shape, 1) % MAP_DIM
    other = jnp.where(lane < half, pltpu.roll(tile, LANES - half, 1), pltpu.roll(tile, half, 1))
    return tile * cosine + other * sine


def groups(cols):
    return max(g for g in (4, 2, 1) if cols % (g * LANES) == 0)


class Plan:
    def __init__(self, L, G):
        self.L, self.G = L, G
        self.first = [X if j < (G + 1) // 2 else Y for j in range(G)]
        self.wide = [G >= 4 and j % 2 == 1 for j in range(G)]
        self.arrival = [{} for _ in range(L)]
        self.issue = [{} for _ in range(L)]
        waiting = {(z, d): [] for z in range(L) for d in range(4)}
        free = dict.fromkeys(waiting, 0.0)
        events, count = [], 0

        def post(time, what):
            nonlocal count
            count += 1
            heapq.heappush(events, (time, count, what))

        def begin(z, d, time):
            while waiting[z, d] and free[z, d] - time < LEAD - 0.01:
                piece = heapq.heappop(waiting[z, d])[-1]
                self.issue[z][piece, d] = time
                free[z, d] = max(time, free[z, d]) + 1
                there, seen = self.beyond(z, piece, d)
                post(free[z, d] + LAG, (there, None, seen))
                post(max(time, free[z, d] - LEAD + 0.02), (z, d, None))

        for z in range(L):
            for m in range(2):
                for j in range(G):
                    post(0.0, (z, None, (m, j, z, 0, 0)))
        while events:
            time, _, (z, d, piece) = heapq.heappop(events)
            if d is not None:
                begin(z, d, time)
                continue
            assert piece not in self.arrival[z]
            self.arrival[z][piece] = time
            for d in self.links(z, piece):
                count += 1
                goes_on = bool(self.links(*self.beyond(z, piece, d)))
                heapq.heappush(waiting[z, d], (self.rank(z, piece, d), count, piece))
            for d in range(4):
                begin(z, d, time)
        self.end = max(max(a.values()) for a in self.arrival)

    def rank(self, z, piece, d):
        m, j, zo, dy, dx = piece
        there, seen = self.beyond(z, piece, d)
        relayed = any(link in (X, Y) for link in self.links(there, seen))
        return m, not relayed

    def outer(self, zo):
        return zo in (0, self.L - 1)

    def links(self, z, piece):
        m, j, zo, dy, dx = piece
        along = [d for d, step in ((UP, 1), (DOWN, -1))
                 if 0 <= z + step < self.L and (z == zo or (step > 0) == (z > zo))]
        second = [X + Y - self.first[j]]
        if (dy, dx) == (0, 0):
            if z == zo or not self.outer(zo):
                return along + [X, Y]
            return along + second * (not self.wide[j])
        if (dx if self.first[j] == X else dy) and not (dx and dy):
            along = along * self.outer(zo)
            return along + second * (z == zo or not self.outer(zo) or not self.wide[j])
        return along * (self.outer(zo) and self.wide[j])

    def beyond(self, z, piece, d):
        m, j, zo, dy, dx = piece
        return z + (d == UP) - (d == DOWN), (m, j, zo, dy ^ (d == Y), dx ^ (d == X))

    def roles(self):
        return range((self.L + 1) // 2)

    def sends(self, k):
        return [(when, p, d) for when, _, (p, d) in sorted(
            (when, i, send) for i, (send, when) in enumerate(self.issue[k].items()))]

    def pieces(self, m, zo, groups, sides=(0, 1)):
        return [(m, j, zo, dy, dx) for j in groups for dy in sides for dx in range(2)]

    def ready(self, k, m, zo, groups, sides=(0, 1)):
        return max(self.arrival[k][p] for p in self.pieces(m, zo, groups, sides))

    def order(self, k, m):
        everything = range(self.G)
        return sorted(range(self.L), key=lambda zo: (zo != k, self.ready(k, m, zo, everything)))


def rows_of(zo, y, depth):
    if 2 * depth % LANES:
        return pl.ds(pl.multiple_of(zo * 4 * depth, 4 * depth), 4 * depth)
    return pl.ds(pl.multiple_of((zo * 4 + y * 2) * depth, 2 * depth), 2 * depth)


def ending(plan, z):
    L, m = plan.L, 1
    role = jnp.minimum(z, L - 1 - z)
    ahead = jnp.where(z <= L - 1 - z, 1, -1)
    zo, ready = z, {j: 0.0 for j in range(plan.G)}
    for k in plan.roles():
        final = plan.order(k, m)[-1]
        zo = jnp.where(role == k, z + ahead * (final - k), zo)
        for j in ready:
            ready[j] = max(ready[j], plan.ready(k, m, final, [j]))
    return role, ahead, zo, [j for j in ready if ready[j] > max(ready.values()) - 0.5]


def kernel(
    n, tp, G, heads, prompt, fresh, wq, wk, wv, lam, gain,
    k_out, v_out, mix_out, gain_out, W, PR, acc,
    fr, XR, XM, wq_v, QS, QP, QT, QR, ct, st, qs, lam_v,
    w_recv, w_send, p_recv, p_send, x_recv, x_send, q_recv, q_send, t_recv, t_send, loc, token,
):
    _, rows, wl = prompt.shape
    depth, cols = wk.shape
    width = cols // G
    L = n // 4
    plane = 4 * depth
    me, mt = lax.axis_index("sp"), lax.axis_index("tp")
    z, y, x = me // 4, (me // 2) % 2, me % 2
    yf, xf = 1 - y, 1 - x
    up_ok, down_ok = z + 1 < L, z > 0
    outer = jnp.logical_not(up_ok & down_ok)

    plan = Plan(L, G)
    role, ahead, last_plane, late = ending(plan, z)

    def at(zo, yo, xo):
        return zo * 4 + yo * 2 + xo

    partner = {X: at(z, y, xf), Y: at(z, yf, x), UP: me + 4, DOWN: me - 4}

    def piece(c, o):
        return W.at[c, pl.ds(pl.multiple_of(o * depth, depth), depth), :]

    target = {X: partner[X], Y: partner[Y], UP: me + 4 * ahead, DOWN: me - 4 * ahead}

    def place(k, p):
        m, j, zo, dy, dx = p
        return m * G + j, at(z + ahead * (zo - k), yf if dy else y, xf if dx else x)

    def copy(c, d, o):
        return pltpu.make_async_remote_copy(
            src_ref=piece(c, o), dst_ref=piece(c, o),
            send_sem=w_send.at[d], recv_sem=w_recv.at[c * n + o],
            device_id={"sp": target[d]}, device_id_type=pl.DeviceIdType.MESH,
        )

    def by_role(f):
        for k in plan.roles():
            pl.when(role == k)(functools.partial(f, k))

    pending = {k: plan.sends(k) for k in plan.roles()}
    arrived = {k: set(plan.pieces(0, k, range(0))) for k in plan.roles()}

    def need(k, p):
        if p[2:] != (k, 0, 0) and p not in arrived[k]:
            arrived[k].add(p)
            c, o = place(k, p)
            copy(c, X, o).wait_recv()

    def advance(time, wanted=lambda k: ()):
        def go(k):
            while pending[k] and pending[k][0][0] < time:
                _, p, d = pending[k].pop(0)
                need(k, p)
                c, o = place(k, p)
                copy(c, d, o).start()
            for p in wanted(k):
                need(k, p)

        by_role(go)

    def loop(lo, hi, f):
        lax.fori_loop(lo, hi, lambda i, _: (f(i), _)[1], 0)

    turns = {(k, m): plan.order(k, m) for k in plan.roles() for m in range(2)}

    def dots(m, t, groups=range(G), sides=(0, 1), last=False):
        zo = z
        for k in plan.roles():
            zo = jnp.where(role == k, z + ahead * (turns[k, m][t] - k), zo)

        R = rows // len(sides)

        def tile(i):
            r = pl.ds(pl.multiple_of(i * R, R), R)
            if len(sides) == 2:
                p = pl.ds(pl.multiple_of(zo * plane, plane), plane)
            else:
                p = rows_of(zo, yf if sides[0] else y, depth)
            for j in groups:
                part = jnp.dot(PR[r, p], W[m * G + j, p, :], preferred_element_type=F32)
                if t > 0 or sides == (1,):
                    part = acc[j, r, :] + part
                if last:
                    v_out[r, pl.ds(j * width, width)] = part.astype(BF16)
                else:
                    acc[j, r, :] = part

        loop(0, rows // R, tile)

    barrier = pltpu.get_barrier_semaphore()

    def cores(which, sem):
        for t in range(tp):
            @pl.when(t > mt if which > 0 else t < mt)
            def _(t=t):
                pl.semaphore_signal(sem, inc=1, device_id={"tp": t}, device_id_type=pl.DeviceIdType.MESH)

    cores(1, barrier)

    def signal(sem, d):
        pl.semaphore_signal(
            sem, inc=1, device_id={"sp": partner[d]}, device_id_type=pl.DeviceIdType.MESH)

    signal(barrier, X)
    signal(barrier, Y)
    pl.when(up_ok)(lambda: signal(barrier, UP))
    pl.when(down_ok)(lambda: signal(barrier, DOWN))

    def columns(t):
        return PR.at[:, pl.ds(pl.multiple_of(t * wl, wl), wl)]

    own = [
        pltpu.make_async_copy(
            w.at[:, pl.ds(j * width, width)], piece(m * G + j, me), loc.at[m])
        for m, w in enumerate((wk, wv)) for j in range(G)
    ]
    rest = [
        pltpu.make_async_copy(src, dst, loc.at[2 + i])
        for i, (src, dst) in enumerate((
            (fresh, fr), (prompt.at[0], columns(mt)), (wq, wq_v), (lam, lam_v), (gain, gain_out)))
    ]

    def own_wait(m):
        whole = W.at[pl.ds(m * G, G), pl.ds(pl.multiple_of(me * depth, depth), depth), :]
        pltpu.make_async_copy(whole, whole, loc.at[m]).wait()

    for c in own[:G]:
        c.start()
    rest[0].start()
    for c in own[G:]:
        c.start()
    for c in rest[1:]:
        c.start()
    own_wait(0)

    pl.semaphore_wait(barrier, 2 + up_ok.astype(jnp.int32) + down_ok.astype(jnp.int32) + mt)

    block_of = XR.shape[2]
    share = wl // depth
    mine = me // share == mt

    def features(chip):
        first_one = (chip * depth) % wl // block_of * block_of
        return pl.ds(pl.multiple_of(first_one, block_of), block_of)

    def x_sends():
        def to(i):
            chip, t = mt * share + (me + i // tp) % share, (mt + i) % tp

            @pl.when((chip != me) | (t != mt))
            def _():
                pltpu.make_async_remote_copy(
                    src_ref=fr.at[:, features(chip)], dst_ref=XR.at[me],
                    send_sem=x_send.at[0], recv_sem=x_recv.at[0],
                    device_id={"sp": chip, "tp": t}, device_id_type=pl.DeviceIdType.MESH,
                ).start()

        loop(0, n, to)

        @pl.when(mine)
        def _():
            XR[me] = fr[:, features(me)]

    def together(ref, send_sem, recv_sem):
        return pltpu.make_async_remote_copy(
            src_ref=ref, dst_ref=ref, send_sem=send_sem.at[0], recv_sem=recv_sem.at[0],
            device_id={"sp": partner[X]}, device_id_type=pl.DeviceIdType.MESH,
        )

    def x_wait(end):
        pl.when(mine)(lambda: end(together(XR.at[pl.ds(0, n - 1)], x_send, x_recv)))
        pl.when(jnp.logical_not(mine))(lambda: end(together(XR, x_send, x_recv)))

    q_all = together(QP.at[pl.ds(0, 3)], q_send, q_recv)
    t_all = together(QR.at[pl.ds(0, L - 1)], t_send, t_recv) if L > 1 else None

    def p_copy(d):
        return pltpu.make_async_remote_copy(
            src_ref=prompt.at[0], dst_ref=columns(mt),
            send_sem=p_send.at[d], recv_sem=p_recv.at[mt],
            device_id={"tp": (mt + d) % tp}, device_id_type=pl.DeviceIdType.MESH,
        )

    def p_wait(d):
        src = (mt + d) % tp
        return pltpu.make_async_remote_copy(
            src_ref=columns(src), dst_ref=columns(src),
            send_sem=p_send.at[d], recv_sem=p_recv.at[src],
            device_id={"tp": src}, device_id_type=pl.DeviceIdType.MESH,
        )

    advance(0.0001)
    cores(-1, token.at[4])

    def relay_token(b):
        for turn, before, more, d in ((z == b, down_ok, up_ok, UP), (z == L - 1 - b, up_ok, down_ok, DOWN)):
            pl.when(turn & before)(lambda d=d: pl.semaphore_wait(token.at[d], 1))
            pl.when(turn & more)(lambda d=d: signal(token.at[d], d))

    rest[0].wait()
    own_wait(1)


    spot = me % 4

    def q_copy(d):
        other = (spot + d) % 4
        return pltpu.make_async_remote_copy(
            src_ref=QS.at[other], dst_ref=QP.at[spot],
            send_sem=q_send.at[0], recv_sem=q_recv.at[0],
            device_id={"sp": z * 4 + other}, device_id_type=pl.DeviceIdType.MESH,
        )

    def t_copy(d):
        other = (z + d) % L
        return pltpu.make_async_remote_copy(
            src_ref=QT.at[other], dst_ref=QR.at[z],
            send_sem=t_send.at[0], recv_sem=t_recv.at[0],
            device_id={"sp": other * 4 + spot}, device_id_type=pl.DeviceIdType.MESH,
        )

    def partial_queries():
        x_wait(lambda c: c.wait_recv())
        for j in range(n):
            XM[pl.ds(j, 1), :] = XR[j].astype(F32)
        chosen = XM[...].astype(BF16)
        if block_of > depth:
            pick = (
                lax.broadcasted_iota(jnp.int32, (block_of, depth), 0)
                == me * depth % block_of + lax.broadcasted_iota(jnp.int32, (block_of, depth), 1)
            )
            chosen = jnp.dot(
                chosen, jnp.where(pick, 1.0, 0.0).astype(BF16), preferred_element_type=F32).astype(BF16)
        rest[2].wait()
        partial = jnp.dot(chosen, wq_v[...], preferred_element_type=F32)
        for j in range(n):
            QS[j % 4, j // 4] = partial[j:j + 1, :]
        QP[spot] = QS[spot]
        loop(1, 4, lambda d: q_copy(d).start())

    def plane_queries():
        q_all.wait_recv()
        QT[...] = (QP[0] + QP[1]) + (QP[2] + QP[3])
        QR[z] = QT[z]
        if L > 1:
            loop(1, L, lambda d: t_copy(d).start())

    hp = max(heads, 8)
    pad = 2 * hp

    def build_query():
        qcos, qsin = table(jnp.full((8, LANES), rows, F32))
        if L > 1:
            t_all.wait_recv()
        total = QR[0]
        for j in range(1, L):
            total = total + QR[j]
        total = jnp.broadcast_to(total, (8, cols))
        query = jnp.concatenate(
            [rotated(total[:, i:i + LANES], qcos, qsin) for i in range(0, cols, LANES)], axis=1)
        query = jnp.broadcast_to(query[:1], (pad, cols))
        row = lax.broadcasted_iota(jnp.int32, (pad, cols), 0)
        keep = 2 * (row % hp) + row // hp == lax.broadcasted_iota(jnp.int32, (pad, cols), 1) // MAP_DIM
        qs[...] = jnp.where(keep, query, 0.0).astype(BF16)

    def angles(i):
        position = (i * 64 + lax.broadcasted_iota(jnp.int32, (64, LANES), 0)).astype(F32)
        r = pl.ds(pl.multiple_of(i * 64, 64), 64)
        ct[r, :], st[r, :] = table(position)

    RR = min(rows, 256)

    def rotate_rows(i):
        r = pl.ds(pl.multiple_of(i * RR, RR), RR)
        cosine, sine = ct[r, :], st[r, :]
        for i in range(0, cols, LANES):
            tile = acc[i // width, r, pl.ds(i % width, LANES)]
            k_out[r, pl.ds(i, LANES)] = rotated(tile, cosine, sine).astype(BF16)

    def weigh():
        scores = lax.dot_general(
            qs[...], k_out[...], (((1,), (1,)), ((), ())), preferred_element_type=F32) * MAP_DIM ** -0.5
        weights = jnp.exp(scores - jnp.max(scores, axis=-1, keepdims=True))
        weights = weights / jnp.sum(weights, axis=-1, keepdims=True)
        rest[3].wait()
        here = (lax.broadcasted_iota(jnp.int32, (hp, heads), 0)
                == lax.broadcasted_iota(jnp.int32, (hp, heads), 1))
        scale = jnp.sum(jnp.where(here, lam_v[...], 0.0), axis=-1, keepdims=True)
        mix = weights[:hp] - scale * weights[hp:]
        high = mix.astype(BF16)
        left = mix - high.astype(F32)
        mid = left.astype(BF16)
        low = (left - mid.astype(F32)).astype(BF16)
        mix_out[...] = jnp.concatenate([high, mid, low], axis=0)

    def when_ready(m, t, groups, sides=(0, 1)):
        return max(plan.ready(k, m, turns[k, m][t], groups, sides) for k in plan.roles())

    def add_dots(when, m, t, groups=range(G), sides=(0, 1), last=False):
        def wanted(k):
            return plan.pieces(m, turns[k, m][t], groups, sides)

        work.append((when, functools.partial(dots, m, t, groups, sides, last), wanted))

    def prompt_whole():
        rest[1].wait()
        for d in range(1, tp):
            p_wait(d).wait_recv()

    def all_cores():
        pl.when(mt < tp - 1)(lambda: pl.semaphore_wait(token.at[4], tp - 1 - mt))
        signal(token.at[Y], Y)
        for d in range(1, tp):
            p_copy(d).start()

    def first_token():
        pl.semaphore_wait(token.at[Y], 1)
        signal(token.at[X], X)

    def second_token():
        pl.semaphore_wait(token.at[X], 1)
        relay_token(0)

    def turn_rows(i):
        loop(i * (rows // RR) // 2, (i + 1) * (rows // RR) // 2, rotate_rows)

    none = lambda k: ()
    work = [
        (TOKC, all_cores, none), (TOK0, first_token, none), (TOK1, second_token, none),
        *((TOK1 + 0.9 * b, functools.partial(relay_token, b), none) for b in range(1, L)),
    ]
    sent_x = TOK1 + 0.9 * L
    work.append((sent_x, x_sends, none))
    work.append((sent_x + 9, partial_queries, none))
    work.append((sent_x + 4, lambda: loop(0, rows // 64, angles), none))
    keys_at = 0
    for m in range(2):
        whole_until = split_until = 0
        for t in range(L):
            when = when_ready(m, t, range(G)) + 0.1 + 0.001 * t
            if m == 0:
                keys_at = max(keys_at, when)
            if (m, t) == (0, 0):
                work.append((when - 0.01, prompt_whole, none))
            if (m, t) == (1, 0):
                when = max(when, keys_at + 2.5)
            when = max(when, whole_until + 0.01)
            if m == 0 or t < max(L - 2, min(1, L - 1)):
                whole_until = when
                keys_at = max(keys_at, when) if m == 0 else keys_at
                add_dots(when, m, t)
                continue
            last, after = t == L - 1, whole_until
            for sides in ([(0,), (1,)] if 2 * depth % LANES == 0 else [(0, 1)]):
                ready = {j: when_ready(m, t, [j], sides) for j in range(G)}
                if not last:
                    parts = [list(range(G))]
                elif sides == (0,):
                    edge = max(ready.values()) - 3
                    parts = [[j for j in ready if ready[j] < edge], [j for j in ready if ready[j] >= edge]]
                else:
                    parts = [[j for j in ready if j not in late]]
                for some in parts:
                    if some:
                        ends = last and 1 in sides
                        after = max(after, max(ready[j] for j in some), split_until if ends else 0) + 0.02
                        split_until = max(split_until, after)
                        add_dots(after, m, t, some, sides, ends)
    work.append((keys_at + 0.1, lambda: turn_rows(0), none))
    work.append((keys_at + 1.3, lambda: turn_rows(1), none))
    work.append((sent_x + 17, plane_queries, none))
    answer = max(sent_x + 17 + 9, keys_at + 2.4)
    work.append((answer, build_query, none))
    work.append((answer + 0.5, weigh, none))
    for time, act, wanted in sorted(work, key=lambda item: item[0]):
        advance(time, wanted)
        act()
    advance(2 * plan.end, lambda k: plan.pieces(1, turns[k, 1][L - 1], late))
    rest[4].wait()
    x_wait(lambda c: c.wait_send())
    q_all.wait_send()
    if L > 1:
        t_all.wait_send()
    for d in range(1, tp):
        p_copy(d).wait_send()

    def sent(d, pieces):
        all_of = W.at[:, pl.ds(0, pieces * depth // G), :]
        pltpu.make_async_remote_copy(
            src_ref=all_of, dst_ref=all_of, send_sem=w_send.at[d], recv_sem=w_recv.at[0],
            device_id={"sp": partner[X]}, device_id_type=pl.DeviceIdType.MESH,
        ).wait_send()

    def settle(k):
        for d in range(4):
            pieces = sum(link == d for _, link in plan.issue[k])
            if pieces:
                sent(d, pieces // 2)

    by_role(settle)


def read(n, G, keys, values, mix, gain, W, PR, acc, k_out, v_out, read_out, fresh, sem):
    hp = mix.shape[0] // 3
    heads = read_out.shape[1]
    depth, width = W.shape[1] // n, W.shape[2]
    me = lax.axis_index("sp")
    _, _, zo, late = ending(Plan(n // 4, G), me // 4)
    k_copy = pltpu.make_async_copy(keys, k_out.at[0], sem.at[0])
    k_copy.start()

    def columns(j):
        return pl.ds(j * width, width)

    source = [fresh if j in late else values for j in range(G)]
    v_copies = [
        pltpu.make_async_copy(source[j].at[:, columns(j)], v_out.at[0, :, columns(j)], sem.at[1 + j])
        for j in range(G)
    ]
    for j in range(G):
        if j not in late:
            v_copies[j].start()
    p = rows_of(zo, 1 - (me // 2) % 2, depth)
    for j in late:
        part = acc[j] + jnp.dot(PR[:, p], W[G + j, p, :], preferred_element_type=F32)
        fresh[:, columns(j)] = part.astype(BF16)
        v_copies[j].start()
    mixed = jnp.concatenate(
        [jnp.dot(mix[...], source[j][:, columns(j)], preferred_element_type=F32) for j in range(G)], axis=1)
    mixed = mixed[:hp] + mixed[hp:2 * hp] + mixed[2 * hp:]
    diff = jnp.concatenate(
        [mixed[h:h + 1, h * VAL_DIM:(h + 1) * VAL_DIM] for h in range(heads)], axis=0)
    normed = diff * lax.rsqrt(jnp.mean(diff * diff, axis=-1, keepdims=True) + norm_eps)
    read_out[0] = (normed * gain[...]).astype(BF16)
    for c in v_copies:
        c.wait()
    k_copy.wait()


def body(n, tp, prompt, new_input, w_query, w_key, w_value, lam, out_gain):
    seqs, rows, wl = prompt.shape
    depth, cols = w_key.shape
    heads = lam.shape[0]
    G = groups(cols)
    hp = max(heads, 8)
    operands = [
        pltpu.with_memory_space_constraint(a, pltpu.HBM)
        for a in (prompt, new_input, w_query, w_key, w_value, lam[None, :], out_gain[None, :])
    ]
    any_ = pl.BlockSpec(memory_space=pl.ANY)
    hbm = pl.BlockSpec(memory_space=pltpu.HBM)
    vmem = pl.BlockSpec(memory_space=pltpu.VMEM)
    dma = pltpu.SemaphoreType.DMA
    keys, values, *passed = pl.pallas_call(
        functools.partial(kernel, n, tp, G, heads),
        out_shape=(
            pltpu.VMEM((rows, cols), BF16),
            pltpu.VMEM((rows, cols), BF16),
            pltpu.VMEM((3 * hp, rows), BF16),
            pltpu.VMEM((1, VAL_DIM), F32),
            pltpu.VMEM((2 * G, n * depth, cols // G), BF16),
            pltpu.VMEM((rows, tp * wl), BF16),
            pltpu.VMEM((G, rows, cols // G), F32),
        ),
        in_specs=[hbm] * 7,
        out_specs=(vmem,) * 7,
        scratch_shapes=[
            pltpu.VMEM((1, wl), BF16),
            pltpu.VMEM((n, 1, max(depth, LANES)), BF16),
            pltpu.VMEM((n, max(depth, LANES)), F32),
            pltpu.VMEM((depth, cols), BF16),
            pltpu.VMEM((4, n // 4, 1, cols), F32),
            pltpu.VMEM((4, n // 4, 1, cols), F32),
            pltpu.VMEM((n // 4, 1, cols), F32),
            pltpu.VMEM((n // 4, 1, cols), F32),
            pltpu.VMEM((rows, LANES), F32),
            pltpu.VMEM((rows, LANES), F32),
            pltpu.VMEM((2 * hp, cols), BF16),
            pltpu.VMEM((1, heads), F32),
            dma((2 * G * n,)), dma((4,)), dma((tp,)), dma((tp,)), dma((1,)), dma((1,)),
            dma((1,)), dma((1,)), dma((1,)), dma((1,)), dma((7,)),
            pltpu.SemaphoreType.REGULAR((5,)),
        ],
        compiler_params=pltpu.CompilerParams(
            collective_id=0, has_side_effects=True, vmem_limit_bytes=20 * 1024 * 1024),
        name="prefill",
    )(*operands)
    return pl.pallas_call(
        functools.partial(read, n, G),
        out_shape=(
            jax.ShapeDtypeStruct((seqs, rows, cols), BF16),
            jax.ShapeDtypeStruct((seqs, rows, cols), BF16),
            jax.ShapeDtypeStruct((seqs, heads, VAL_DIM), BF16),
        ),
        in_specs=[vmem] * 7,
        out_specs=(any_, any_, vmem),
        scratch_shapes=[pltpu.VMEM((rows, cols), BF16), dma((1 + G,))],
        compiler_params=pltpu.CompilerParams(vmem_limit_bytes=24 * 1024 * 1024),
        name="read",
    )(keys, values, *passed)


def solution(mesh):
    in_specs = (
        P("sp", None, "tp"), P("sp", "tp"), P("sp", "tp"), P("sp", "tp"), P("sp", "tp"), P("tp"), P(),
    )
    out_specs = (P("sp", None, "tp"), P("sp", None, "tp"), P("sp", "tp", None))
    return jax.shard_map(
        functools.partial(body, mesh.shape["sp"], mesh.shape["tp"]),
        mesh=mesh, in_specs=in_specs, out_specs=out_specs, check_vma=False)
```

```python
import functools
import heapq
import math

import jax
import jax.numpy as jnp
from jax import lax
from jax.experimental import pallas as pl
from jax.experimental.pallas import tpu as pltpu
from jax.sharding import PartitionSpec as P

MAP_DIM = 64
VAL_DIM = 128
LANES = 128
rope_base = 500000.0
norm_eps = 1e-05

X, Y, UP, DOWN = 0, 1, 2, 3
LAG, LEAD = 0.9, 2.0
TOKC, TOK0, TOK1 = 1.0, 2.5, 4.0
F32, BF16 = jnp.float32, jnp.bfloat16


def inverse_freq(shape):
    lane = lax.broadcasted_iota(jnp.int32, shape, 1) % (MAP_DIM // 2)
    return jnp.exp(lane.astype(F32) * (-2.0 / MAP_DIM * math.log(rope_base)))


def table(position):
    angle = position * inverse_freq(position.shape)
    lane = lax.broadcasted_iota(jnp.int32, angle.shape, 1) % MAP_DIM
    sine = jnp.sin(angle)
    return jnp.cos(angle), jnp.where(lane < MAP_DIM // 2, -sine, sine)


def rotated(tile, cosine, sine):
    half = MAP_DIM // 2
    lane = lax.broadcasted_iota(jnp.int32, tile.shape, 1) % MAP_DIM
    other = jnp.where(lane < half, pltpu.roll(tile, LANES - half, 1), pltpu.roll(tile, half, 1))
    return tile * cosine + other * sine


def groups(cols):
    return max(g for g in (4, 2, 1) if cols % (g * LANES) == 0)


class Plan:
    def __init__(self, L, G):
        self.L, self.G = L, G
        self.first = [X if j < (G + 1) // 2 else Y for j in range(G)]
        self.wide = [G >= 4 and j % 2 == 1 for j in range(G)]
        self.arrival = [{} for _ in range(L)]
        self.issue = [{} for _ in range(L)]
        waiting = {(z, d): [] for z in range(L) for d in range(4)}
        free = dict.fromkeys(waiting, 0.0)
        events, count = [], 0

        def post(time, what):
            nonlocal count
            count += 1
            heapq.heappush(events, (time, count, what))

        def begin(z, d, time):
            while waiting[z, d] and free[z, d] - time < LEAD - 0.01:
                piece = heapq.heappop(waiting[z, d])[-1]
                self.issue[z][piece, d] = time
                free[z, d] = max(time, free[z, d]) + 1
                there, seen = self.beyond(z, piece, d)
                post(free[z, d] + LAG, (there, None, seen))
                post(max(time, free[z, d] - LEAD + 0.02), (z, d, None))

        for z in range(L):
            for m in range(2):
                for j in range(G):
                    post(0.0, (z, None, (m, j, z, 0, 0)))
        while events:
            time, _, (z, d, piece) = heapq.heappop(events)
            if d is not None:
                begin(z, d, time)
                continue
            assert piece not in self.arrival[z]
            self.arrival[z][piece] = time
            for d in self.links(z, piece):
                count += 1
                goes_on = bool(self.links(*self.beyond(z, piece, d)))
                heapq.heappush(waiting[z, d], (self.rank(z, piece, d), count, piece))
            for d in range(4):
                begin(z, d, time)
        self.end = max(max(a.values()) for a in self.arrival)

    def rank(self, z, piece, d):
        m, j, zo, dy, dx = piece
        there, seen = self.beyond(z, piece, d)
        relayed = any(link in (X, Y) for link in self.links(there, seen))
        return m, not relayed

    def outer(self, zo):
        return zo in (0, self.L - 1)

    def links(self, z, piece):
        m, j, zo, dy, dx = piece
        along = [d for d, step in ((UP, 1), (DOWN, -1))
                 if 0 <= z + step < self.L and (z == zo or (step > 0) == (z > zo))]
        second = [X + Y - self.first[j]]
        if (dy, dx) == (0, 0):
            if z == zo or not self.outer(zo):
                return along + [X, Y]
            return along + second * (not self.wide[j])
        if (dx if self.first[j] == X else dy) and not (dx and dy):
            along = along * self.outer(zo)
            return along + second * (z == zo or not self.outer(zo) or not self.wide[j])
        return along * (self.outer(zo) and self.wide[j])

    def beyond(self, z, piece, d):
        m, j, zo, dy, dx = piece
        return z + (d == UP) - (d == DOWN), (m, j, zo, dy ^ (d == Y), dx ^ (d == X))

    def roles(self):
        return range((self.L + 1) // 2)

    def sends(self, k):
        return [(when, p, d) for when, _, (p, d) in sorted(
            (when, i, send) for i, (send, when) in enumerate(self.issue[k].items()))]

    def pieces(self, m, zo, groups, sides=(0, 1)):
        return [(m, j, zo, dy, dx) for j in groups for dy in sides for dx in range(2)]

    def ready(self, k, m, zo, groups, sides=(0, 1)):
        return max(self.arrival[k][p] for p in self.pieces(m, zo, groups, sides))

    def order(self, k, m):
        everything = range(self.G)
        return sorted(range(self.L), key=lambda zo: (zo != k, self.ready(k, m, zo, everything)))


def rows_of(zo, y, depth):
    if 2 * depth % LANES:
        return pl.ds(pl.multiple_of(zo * 4 * depth, 4 * depth), 4 * depth)
    return pl.ds(pl.multiple_of((zo * 4 + y * 2) * depth, 2 * depth), 2 * depth)


def ending(plan, z):
    L, m = plan.L, 1
    role = jnp.minimum(z, L - 1 - z)
    ahead = jnp.where(z <= L - 1 - z, 1, -1)
    zo, ready = z, {j: 0.0 for j in range(plan.G)}
    for k in plan.roles():
        final = plan.order(k, m)[-1]
        zo = jnp.where(role == k, z + ahead * (final - k), zo)
        for j in ready:
            ready[j] = max(ready[j], plan.ready(k, m, final, [j]))
    return role, ahead, zo, [j for j in ready if ready[j] > max(ready.values()) - 0.5]


def kernel(
    n, tp, G, heads, prompt, fresh, wq, wk, wv, lam, gain,
    k_out, v_out, mix_out, gain_out, W, PR, acc,
    fr, XR, XM, wq_v, QS, QP, QT, QR, ct, st, qs, lam_v,
    w_recv, w_send, p_recv, p_send, x_recv, x_send, q_recv, q_send, t_recv, t_send, loc, token,
):
    _, rows, wl = prompt.shape
    depth, cols = wk.shape
    width = cols // G
    L = n // 4
    plane = 4 * depth
    me, mt = lax.axis_index("sp"), lax.axis_index("tp")
    z, y, x = me // 4, (me // 2) % 2, me % 2
    yf, xf = 1 - y, 1 - x
    up_ok, down_ok = z + 1 < L, z > 0
    outer = jnp.logical_not(up_ok & down_ok)

    plan = Plan(L, G)
    role, ahead, last_plane, late = ending(plan, z)

    def at(zo, yo, xo):
        return zo * 4 + yo * 2 + xo

    partner = {X: at(z, y, xf), Y: at(z, yf, x), UP: me + 4, DOWN: me - 4}

    def piece(c, o):
        return W.at[c, pl.ds(pl.multiple_of(o * depth, depth), depth), :]

    target = {X: partner[X], Y: partner[Y], UP: me + 4 * ahead, DOWN: me - 4 * ahead}

    def place(k, p):
        m, j, zo, dy, dx = p
        return m * G + j, at(z + ahead * (zo - k), yf if dy else y, xf if dx else x)

    def copy(c, d, o):
        return pltpu.make_async_remote_copy(
            src_ref=piece(c, o), dst_ref=piece(c, o),
            send_sem=w_send.at[d], recv_sem=w_recv.at[c * n + o],
            device_id={"sp": target[d]}, device_id_type=pl.DeviceIdType.MESH,
        )

    def by_role(f):
        for k in plan.roles():
            pl.when(role == k)(functools.partial(f, k))

    pending = {k: plan.sends(k) for k in plan.roles()}
    arrived = {k: set(plan.pieces(0, k, range(0))) for k in plan.roles()}

    def need(k, p):
        if p[2:] != (k, 0, 0) and p not in arrived[k]:
            arrived[k].add(p)
            c, o = place(k, p)
            copy(c, X, o).wait_recv()

    def advance(time, wanted=lambda k: ()):
        def go(k):
            while pending[k] and pending[k][0][0] < time:
                _, p, d = pending[k].pop(0)
                need(k, p)
                c, o = place(k, p)
                copy(c, d, o).start()
            for p in wanted(k):
                need(k, p)

        by_role(go)

    def loop(lo, hi, f):
        lax.fori_loop(lo, hi, lambda i, _: (f(i), _)[1], 0)

    turns = {(k, m): plan.order(k, m) for k in plan.roles() for m in range(2)}

    def dots(m, t, groups=range(G), sides=(0, 1), last=False):
        zo = z
        for k in plan.roles():
            zo = jnp.where(role == k, z + ahead * (turns[k, m][t] - k), zo)

        R = rows // len(sides)

        def tile(i):
            r = pl.ds(pl.multiple_of(i * R, R), R)
            if len(sides) == 2:
                p = pl.ds(pl.multiple_of(zo * plane, plane), plane)
            else:
                p = rows_of(zo, yf if sides[0] else y, depth)
            for j in groups:
                part = jnp.dot(PR[r, p], W[m * G + j, p, :], preferred_element_type=F32)
                if t > 0 or sides == (1,):
                    part = acc[j, r, :] + part
                if last:
                    v_out[r, pl.ds(j * width, width)] = part.astype(BF16)
                else:
                    acc[j, r, :] = part

        loop(0, rows // R, tile)

    barrier = pltpu.get_barrier_semaphore()

    def cores(which, sem):
        for t in range(tp):
            @pl.when(t > mt if which > 0 else t < mt)
            def _(t=t):
                pl.semaphore_signal(sem, inc=1, device_id={"tp": t}, device_id_type=pl.DeviceIdType.MESH)

    cores(1, barrier)

    def signal(sem, d):
        pl.semaphore_signal(
            sem, inc=1, device_id={"sp": partner[d]}, device_id_type=pl.DeviceIdType.MESH)

    signal(barrier, X)
    signal(barrier, Y)
    pl.when(up_ok)(lambda: signal(barrier, UP))
    pl.when(down_ok)(lambda: signal(barrier, DOWN))

    def columns(t):
        return PR.at[:, pl.ds(pl.multiple_of(t * wl, wl), wl)]

    own = [
        pltpu.make_async_copy(
            w.at[:, pl.ds(j * width, width)], piece(m * G + j, me), loc.at[m])
        for m, w in enumerate((wk, wv)) for j in range(G)
    ]
    rest = [
        pltpu.make_async_copy(src, dst, loc.at[2 + i])
        for i, (src, dst) in enumerate((
            (fresh, fr), (prompt.at[0], columns(mt)), (wq, wq_v), (lam, lam_v), (gain, gain_out)))
    ]

    def own_wait(m):
        whole = W.at[pl.ds(m * G, G), pl.ds(pl.multiple_of(me * depth, depth), depth), :]
        pltpu.make_async_copy(whole, whole, loc.at[m]).wait()

    for c in own[:G]:
        c.start()
    rest[0].start()
    for c in own[G:]:
        c.start()
    for c in rest[1:]:
        c.start()
    own_wait(0)

    pl.semaphore_wait(barrier, 2 + up_ok.astype(jnp.int32) + down_ok.astype(jnp.int32) + mt)

    block_of = XR.shape[2]
    share = wl // depth
    mine = me // share == mt

    def features(chip):
        first_one = (chip * depth) % wl // block_of * block_of
        return pl.ds(pl.multiple_of(first_one, block_of), block_of)

    def x_sends():
        def to(i):
            chip, t = mt * share + (me + i // tp) % share, (mt + i) % tp

            @pl.when((chip != me) | (t != mt))
            def _():
                pltpu.make_async_remote_copy(
                    src_ref=fr.at[:, features(chip)], dst_ref=XR.at[me],
                    send_sem=x_send.at[0], recv_sem=x_recv.at[0],
                    device_id={"sp": chip, "tp": t}, device_id_type=pl.DeviceIdType.MESH,
                ).start()

        loop(0, n, to)

        @pl.when(mine)
        def _():
            XR[me] = fr[:, features(me)]

    def together(ref, send_sem, recv_sem):
        return pltpu.make_async_remote_copy(
            src_ref=ref, dst_ref=ref, send_sem=send_sem.at[0], recv_sem=recv_sem.at[0],
            device_id={"sp": partner[X]}, device_id_type=pl.DeviceIdType.MESH,
        )

    def x_wait(end):
        pl.when(mine)(lambda: end(together(XR.at[pl.ds(0, n - 1)], x_send, x_recv)))
        pl.when(jnp.logical_not(mine))(lambda: end(together(XR, x_send, x_recv)))

    q_all = together(QP.at[pl.ds(0, 3)], q_send, q_recv)
    t_all = together(QR.at[pl.ds(0, L - 1)], t_send, t_recv) if L > 1 else None

    def p_copy(d):
        return pltpu.make_async_remote_copy(
            src_ref=prompt.at[0], dst_ref=columns(mt),
            send_sem=p_send.at[d], recv_sem=p_recv.at[mt],
            device_id={"tp": (mt + d) % tp}, device_id_type=pl.DeviceIdType.MESH,
        )

    def p_wait(d):
        src = (mt + d) % tp
        return pltpu.make_async_remote_copy(
            src_ref=columns(src), dst_ref=columns(src),
            send_sem=p_send.at[d], recv_sem=p_recv.at[src],
            device_id={"tp": src}, device_id_type=pl.DeviceIdType.MESH,
        )

    advance(0.0001)
    cores(-1, token.at[4])

    def relay_token(b):
        for turn, before, more, d in ((z == b, down_ok, up_ok, UP), (z == L - 1 - b, up_ok, down_ok, DOWN)):
            pl.when(turn & before)(lambda d=d: pl.semaphore_wait(token.at[d], 1))
            pl.when(turn & more)(lambda d=d: signal(token.at[d], d))

    rest[0].wait()
    own_wait(1)


    spot = me % 4

    def q_copy(d):
        other = (spot + d) % 4
        return pltpu.make_async_remote_copy(
            src_ref=QS.at[other], dst_ref=QP.at[spot],
            send_sem=q_send.at[0], recv_sem=q_recv.at[0],
            device_id={"sp": z * 4 + other}, device_id_type=pl.DeviceIdType.MESH,
        )

    def t_copy(d):
        other = (z + d) % L
        return pltpu.make_async_remote_copy(
            src_ref=QT.at[other], dst_ref=QR.at[z],
            send_sem=t_send.at[0], recv_sem=t_recv.at[0],
            device_id={"sp": other * 4 + spot}, device_id_type=pl.DeviceIdType.MESH,
        )

    def partial_queries():
        x_wait(lambda c: c.wait_recv())
        for j in range(n):
            XM[pl.ds(j, 1), :] = XR[j].astype(F32)
        chosen = XM[...].astype(BF16)
        if block_of > depth:
            pick = (
                lax.broadcasted_iota(jnp.int32, (block_of, depth), 0)
                == me * depth % block_of + lax.broadcasted_iota(jnp.int32, (block_of, depth), 1)
            )
            chosen = jnp.dot(
                chosen, jnp.where(pick, 1.0, 0.0).astype(BF16), preferred_element_type=F32).astype(BF16)
        rest[2].wait()
        partial = jnp.dot(chosen, wq_v[...], preferred_element_type=F32)
        for j in range(n):
            QS[j % 4, j // 4] = partial[j:j + 1, :]
        QP[spot] = QS[spot]
        loop(1, 4, lambda d: q_copy(d).start())

    def plane_queries():
        q_all.wait_recv()
        QT[...] = (QP[0] + QP[1]) + (QP[2] + QP[3])
        QR[z] = QT[z]
        if L > 1:
            loop(1, L, lambda d: t_copy(d).start())

    hp = max(heads, 8)
    pad = 2 * hp

    def build_query():
        qcos, qsin = table(jnp.full((8, LANES), rows, F32))
        if L > 1:
            t_all.wait_recv()
        total = QR[0]
        for j in range(1, L):
            total = total + QR[j]
        total = jnp.broadcast_to(total, (8, cols))
        query = jnp.concatenate(
            [rotated(total[:, i:i + LANES], qcos, qsin) for i in range(0, cols, LANES)], axis=1)
        query = jnp.broadcast_to(query[:1], (pad, cols))
        row = lax.broadcasted_iota(jnp.int32, (pad, cols), 0)
        keep = 2 * (row % hp) + row // hp == lax.broadcasted_iota(jnp.int32, (pad, cols), 1) // MAP_DIM
        qs[...] = jnp.where(keep, query, 0.0).astype(BF16)

    def angles(i):
        position = (i * 64 + lax.broadcasted_iota(jnp.int32, (64, LANES), 0)).astype(F32)
        r = pl.ds(pl.multiple_of(i * 64, 64), 64)
        ct[r, :], st[r, :] = table(position)

    RR = min(rows, 256)

    def rotate_rows(i):
        r = pl.ds(pl.multiple_of(i * RR, RR), RR)
        cosine, sine = ct[r, :], st[r, :]
        for i in range(0, cols, LANES):
            tile = acc[i // width, r, pl.ds(i % width, LANES)]
            k_out[r, pl.ds(i, LANES)] = rotated(tile, cosine, sine).astype(BF16)

    def weigh():
        scores = lax.dot_general(
            qs[...], k_out[...], (((1,), (1,)), ((), ())), preferred_element_type=F32) * MAP_DIM ** -0.5
        weights = jnp.exp(scores - jnp.max(scores, axis=-1, keepdims=True))
        weights = weights / jnp.sum(weights, axis=-1, keepdims=True)
        rest[3].wait()
        here = (lax.broadcasted_iota(jnp.int32, (hp, heads), 0)
                == lax.broadcasted_iota(jnp.int32, (hp, heads), 1))
        scale = jnp.sum(jnp.where(here, lam_v[...], 0.0), axis=-1, keepdims=True)
        mix = weights[:hp] - scale * weights[hp:]
        high = mix.astype(BF16)
        left = mix - high.astype(F32)
        mid = left.astype(BF16)
        low = (left - mid.astype(F32)).astype(BF16)
        mix_out[...] = jnp.concatenate([high, mid, low], axis=0)

    def when_ready(m, t, groups, sides=(0, 1)):
        return max(plan.ready(k, m, turns[k, m][t], groups, sides) for k in plan.roles())

    def add_dots(when, m, t, groups=range(G), sides=(0, 1), last=False):
        def wanted(k):
            return plan.pieces(m, turns[k, m][t], groups, sides)

        work.append((when, functools.partial(dots, m, t, groups, sides, last), wanted))

    def prompt_whole():
        rest[1].wait()
        for d in range(1, tp):
            p_wait(d).wait_recv()

    def all_cores():
        pl.when(mt < tp - 1)(lambda: pl.semaphore_wait(token.at[4], tp - 1 - mt))
        signal(token.at[Y], Y)
        for d in range(1, tp):
            p_copy(d).start()

    def first_token():
        pl.semaphore_wait(token.at[Y], 1)
        signal(token.at[X], X)

    def second_token():
        pl.semaphore_wait(token.at[X], 1)
        relay_token(0)

    def turn_rows(i):
        loop(i * (rows // RR) // 2, (i + 1) * (rows // RR) // 2, rotate_rows)

    none = lambda k: ()
    work = [
        (TOKC, all_cores, none), (TOK0, first_token, none), (TOK1, second_token, none),
        *((TOK1 + 0.9 * b, functools.partial(relay_token, b), none) for b in range(1, L)),
    ]
    sent_x = TOK1 + 0.9 * L
    work.append((sent_x, x_sends, none))
    work.append((sent_x + 9, partial_queries, none))
    work.append((sent_x + 4, lambda: loop(0, rows // 64, angles), none))
    keys_at = 0
    for m in range(2):
        whole_until = split_until = 0
        for t in range(L):
            when = when_ready(m, t, range(G)) + 0.1 + 0.001 * t
            if m == 0:
                keys_at = max(keys_at, when)
            if (m, t) == (0, 0):
                work.append((when - 0.01, prompt_whole, none))
            if (m, t) == (1, 0):
                when = max(when, keys_at + 2.5)
            when = max(when, whole_until + 0.01)
            if m == 0 or t < max(L - 2, min(1, L - 1)):
                whole_until = when
                keys_at = max(keys_at, when) if m == 0 else keys_at
                add_dots(when, m, t)
                continue
            last, after = t == L - 1, whole_until
            for sides in ([(0,), (1,)] if 2 * depth % LANES == 0 else [(0, 1)]):
                ready = {j: when_ready(m, t, [j], sides) for j in range(G)}
                if not last:
                    parts = [list(range(G))]
                elif sides == (0,):
                    edge = max(ready.values()) - 3
                    parts = [[j for j in ready if ready[j] < edge], [j for j in ready if ready[j] >= edge]]
                else:
                    parts = [[j for j in ready if j not in late]]
                for some in parts:
                    if some:
                        ends = last and 1 in sides
                        after = max(after, max(ready[j] for j in some), split_until if ends else 0) + 0.02
                        split_until = max(split_until, after)
                        add_dots(after, m, t, some, sides, ends)
    work.append((keys_at + 0.1, lambda: turn_rows(0), none))
    work.append((keys_at + 1.3, lambda: turn_rows(1), none))
    work.append((sent_x + 17, plane_queries, none))
    answer = max(sent_x + 17 + 9, keys_at + 2.4)
    work.append((answer, build_query, none))
    work.append((answer + 0.5, weigh, none))
    for time, act, wanted in sorted(work, key=lambda item: item[0]):
        advance(time, wanted)
        act()
    advance(2 * plan.end, lambda k: plan.pieces(1, turns[k, 1][L - 1], late))
    rest[4].wait()
    x_wait(lambda c: c.wait_send())
    q_all.wait_send()
    if L > 1:
        t_all.wait_send()
    for d in range(1, tp):
        p_copy(d).wait_send()

    def sent(d, pieces):
        all_of = W.at[:, pl.ds(0, pieces * depth // G), :]
        pltpu.make_async_remote_copy(
            src_ref=all_of, dst_ref=all_of, send_sem=w_send.at[d], recv_sem=w_recv.at[0],
            device_id={"sp": partner[X]}, device_id_type=pl.DeviceIdType.MESH,
        ).wait_send()

    def settle(k):
        for d in range(4):
            pieces = sum(link == d for _, link in plan.issue[k])
            if pieces:
                sent(d, pieces // 2)

    by_role(settle)


def read(n, G, keys, values, mix, gain, W, PR, acc, k_out, v_out, read_out, fresh, answer, sem):
    hp = mix.shape[0] // 3
    heads = read_out.shape[1]
    depth, width = W.shape[1] // n, W.shape[2]
    me = lax.axis_index("sp")
    _, _, zo, late = ending(Plan(n // 4, G), me // 4)
    k_copy = pltpu.make_async_copy(keys, k_out.at[0], sem.at[0])
    k_copy.start()

    def columns(j):
        return pl.ds(j * width, width)

    source = [fresh if j in late else values for j in range(G)]
    v_copies = [
        pltpu.make_async_copy(source[j].at[:, columns(j)], v_out.at[0, :, columns(j)], sem.at[1 + j])
        for j in range(G)
    ]
    for j in range(G):
        if j not in late:
            v_copies[j].start()
    p = rows_of(zo, 1 - (me // 2) % 2, depth)
    for j in late:
        part = acc[j] + jnp.dot(PR[:, p], W[G + j, p, :], preferred_element_type=F32)
        fresh[:, columns(j)] = part.astype(BF16)
        v_copies[j].start()
    mixed = jnp.concatenate(
        [jnp.dot(mix[...], source[j][:, columns(j)], preferred_element_type=F32) for j in range(G)], axis=1)
    mixed = mixed[:hp] + mixed[hp:2 * hp] + mixed[2 * hp:]
    diff = jnp.concatenate(
        [mixed[h:h + 1, h * VAL_DIM:(h + 1) * VAL_DIM] for h in range(heads)], axis=0)
    normed = diff * lax.rsqrt(jnp.mean(diff * diff, axis=-1, keepdims=True) + norm_eps)
    answer[0] = (normed * gain[...]).astype(BF16)
    r_copy = pltpu.make_async_copy(answer, read_out, sem.at[1 + G])
    r_copy.start()
    for c in v_copies:
        c.wait()
    k_copy.wait()
    r_copy.wait()


def body(n, tp, prompt, new_input, w_query, w_key, w_value, lam, out_gain):
    seqs, rows, wl = prompt.shape
    depth, cols = w_key.shape
    heads = lam.shape[0]
    G = groups(cols)
    hp = max(heads, 8)
    operands = [
        pltpu.with_memory_space_constraint(a, pltpu.HBM)
        for a in (prompt, new_input, w_query, w_key, w_value, lam[None, :], out_gain[None, :])
    ]
    any_ = pl.BlockSpec(memory_space=pl.ANY)
    hbm = pl.BlockSpec(memory_space=pltpu.HBM)
    vmem = pl.BlockSpec(memory_space=pltpu.VMEM)
    dma = pltpu.SemaphoreType.DMA
    keys, values, *passed = pl.pallas_call(
        functools.partial(kernel, n, tp, G, heads),
        out_shape=(
            pltpu.VMEM((rows, cols), BF16),
            pltpu.VMEM((rows, cols), BF16),
            pltpu.VMEM((3 * hp, rows), BF16),
            pltpu.VMEM((1, VAL_DIM), F32),
            pltpu.VMEM((2 * G, n * depth, cols // G), BF16),
            pltpu.VMEM((rows, tp * wl), BF16),
            pltpu.VMEM((G, rows, cols // G), F32),
        ),
        in_specs=[hbm] * 7,
        out_specs=(vmem,) * 7,
        scratch_shapes=[
            pltpu.VMEM((1, wl), BF16),
            pltpu.VMEM((n, 1, max(depth, LANES)), BF16),
            pltpu.VMEM((n, max(depth, LANES)), F32),
            pltpu.VMEM((depth, cols), BF16),
            pltpu.VMEM((4, n // 4, 1, cols), F32),
            pltpu.VMEM((4, n // 4, 1, cols), F32),
            pltpu.VMEM((n // 4, 1, cols), F32),
            pltpu.VMEM((n // 4, 1, cols), F32),
            pltpu.VMEM((rows, LANES), F32),
            pltpu.VMEM((rows, LANES), F32),
            pltpu.VMEM((2 * hp, cols), BF16),
            pltpu.VMEM((1, heads), F32),
            dma((2 * G * n,)), dma((4,)), dma((tp,)), dma((tp,)), dma((1,)), dma((1,)),
            dma((1,)), dma((1,)), dma((1,)), dma((1,)), dma((7,)),
            pltpu.SemaphoreType.REGULAR((5,)),
        ],
        compiler_params=pltpu.CompilerParams(
            collective_id=0, has_side_effects=True, vmem_limit_bytes=20 * 1024 * 1024),
        name="prefill",
    )(*operands)
    return pl.pallas_call(
        functools.partial(read, n, G),
        out_shape=(
            jax.ShapeDtypeStruct((seqs, rows, cols), BF16),
            jax.ShapeDtypeStruct((seqs, rows, cols), BF16),
            jax.ShapeDtypeStruct((seqs, heads, VAL_DIM), BF16),
        ),
        in_specs=[vmem] * 7,
        out_specs=(any_, any_, any_),
        scratch_shapes=[
            pltpu.VMEM((rows, cols), BF16), pltpu.VMEM((1, heads, VAL_DIM), BF16), dma((2 + G,))],
        compiler_params=pltpu.CompilerParams(vmem_limit_bytes=24 * 1024 * 1024),
        name="read",
    )(keys, values, *passed)


def solution(mesh):
    in_specs = (
        P("sp", None, "tp"), P("sp", "tp"), P("sp", "tp"), P("sp", "tp"), P("sp", "tp"), P("tp"), P(),
    )
    out_specs = (P("sp", None, "tp"), P("sp", None, "tp"), P("sp", "tp", None))
    return jax.shard_map(
        functools.partial(body, mesh.shape["sp"], mesh.shape["tp"]),
        mesh=mesh, in_specs=in_specs, out_specs=out_specs, check_vma=False)
```
